256 devices in a mesh: rep: 32 (over z, y), fs: 4 (over x), tp: 2 (over core).
Axes of the slice: x: 4, y: 4, z: 8, core: 2. Of those that a mesh axis runs over, the one named last changes fastest.
Arguments:
- tokens: bfloat16 [32768, 2048], P(('rep', 'fs', 'tp')), may hold values from -24 to 24
- cotangent: bfloat16 [32768, 2048], P(('rep', 'fs', 'tp')), may hold values from -24 to 24
- gate_weight: bfloat16 [2048, 3072], P(None, 'fs'), may hold values from -0.125 to 0.125
- up_weight: bfloat16 [2048, 3072], P(None, 'fs'), may hold values from -0.125 to 0.125
- down_weight_t: bfloat16 [2048, 3072], P(None, 'fs'), may hold values from -0.109375 to 0.109375
Outputs:
- input_grad: bfloat16 [32768, 2048], P(('rep', 'fs', 'tp'))
- gate_grad: float32 [2048, 3072], P(('rep', 'tp'), 'fs')
- up_grad: float32 [2048, 3072], P(('rep', 'tp'), 'fs')
- down_grad: float32 [2048, 3072], P(('rep', 'tp'), 'fs')
The draws below stay inside these ranges and needn't reach their ends.
All inputs are finite; a program needn't handle non-finite values.
Results may differ from the reference program's by a relative error of at most 0.012.
Values may be sent and summed in bfloat16 or wider, within the bound.
A program may use at most 128 MiB of HBM per device.

```python
import jax
import jax.numpy as jnp
from jax import lax

D = 2048
FF = 3072
TOKENS = 32768
N_REP = 32
N_FS = 4


def raised(result, rng, source, target, blocks, factor):
    def block_of(axis_at):
        return (jnp.arange(result.shape[axis_at]) // (result.shape[axis_at] // blocks)).reshape((-1,) + (1,) * (result.ndim - 1 - axis_at))

    first = jax.random.permutation(rng, blocks)[block_of(target)]
    other_side = (block_of(target) + blocks // 2) % blocks
    return jnp.where((block_of(source) == first) | (block_of(source) == other_side), factor * result, result)


def block_levels(rng, shape, shards, low, top_value):
    def one(dim, shards_of):
        heights = jax.random.uniform(jax.random.fold_in(jax.random.fold_in(rng, 6), dim), (shards_of,), jnp.float32, low / len(shards), top_value / len(shards))
        return jnp.repeat(jnp.exp(heights), shape[dim] // shards_of).reshape((-1,) + (1,) * (len(shape) - dim - 1))

    loudness = one(*shards[0])
    for cut in shards[1:]:
        loudness = loudness * one(*cut)
    return loudness


def gaussian(key, extent, width, limit, split=(), kind=jnp.bfloat16):
    loudness = block_levels(key, extent, split, -0.22, 0.18) if split else 1.0
    result = jax.random.normal(key, extent, jnp.float32) * width * loudness
    return jnp.minimum(jnp.maximum(result, -limit), limit).astype(kind)


def noise_with(key, dims, width, most, pieces, heavy, held_as=jnp.bfloat16):
    values = width * jax.random.normal(key, dims, jnp.float32)
    if pieces:
        values = values * block_levels(key, dims, pieces, -0.22, 0.18)
    return jnp.clip(raised(values, jax.random.fold_in(key, 3), *heavy), -most, most).astype(held_as)


def setup_inputs(seed: int = 0) -> dict:
    arg_keys = jax.random.split(jax.random.key(seed), 6)
    tokens = noise_with(arg_keys[0], (TOKENS, D), 1.0, 24.0, ((0, 256),), (0, 1, 256, 6.0))
    cotangent = noise_with(arg_keys[1], (TOKENS, D), 1.0, 24.0, ((0, 256),), (0, 1, 256, 6.0))
    gate_weight = gaussian(arg_keys[2], (D, FF), D ** -0.5, 0.125, ((1, 4),))
    up_weight = gaussian(arg_keys[3], (D, FF), D ** -0.5, 0.125, ((1, 4),))
    down_weight_t = gaussian(arg_keys[4], (D, FF), FF ** -0.5, 0.109375, ((1, 4),))
    return dict(tokens=tokens, cotangent=cotangent, gate_weight=gate_weight, up_weight=up_weight, down_weight_t=down_weight_t)


def reference(tokens, cotangent, gate_weight, up_weight, down_weight_t):
    row_block = TOKENS // N_REP
    hid_width = FF // N_FS
    gate_split = gate_weight.astype(jnp.float32).reshape(D, N_FS, hid_width)
    up_split = up_weight.astype(jnp.float32).reshape(D, N_FS, hid_width)

    def accumulate(totals, block_index):
        first_row = block_index * row_block
        tok_rows = lax.dynamic_slice_in_dim(tokens, first_row, row_block, 0)
        cot_rows = lax.dynamic_slice_in_dim(cotangent, first_row, row_block, 0)
        gate_pre = jnp.dot(tok_rows, gate_weight, preferred_element_type=jnp.float32)
        up_pre = jnp.dot(tok_rows, up_weight, preferred_element_type=jnp.float32)
        sig_gate = jax.nn.sigmoid(gate_pre)
        act_gate = gate_pre * sig_gate
        hidden = (act_gate * up_pre).astype(jnp.bfloat16)
        hid_grad = jnp.dot(cot_rows, down_weight_t, preferred_element_type=jnp.float32)
        gate_back = (hid_grad * up_pre * sig_gate * (1.0 + gate_pre * (1.0 - sig_gate))).astype(jnp.bfloat16)
        up_back = (hid_grad * act_gate).astype(jnp.bfloat16)
        partial_value = jnp.einsum("rnf,dnf->nrd", gate_back.astype(jnp.float32).reshape(row_block, N_FS, hid_width),
                             gate_split, precision=lax.Precision.HIGHEST)
        partial_value = partial_value + jnp.einsum("rnf,dnf->nrd", up_back.astype(jnp.float32).reshape(row_block, N_FS, hid_width),
                                       up_split, precision=lax.Precision.HIGHEST)
        rounded = lax.optimization_barrier(partial_value.astype(jnp.bfloat16))
        input_rows = jnp.sum(rounded.astype(jnp.float32), axis=0).astype(jnp.bfloat16)
        new_totals = (totals[0] + jnp.dot(tok_rows.T, gate_back, preferred_element_type=jnp.float32),
                      totals[1] + jnp.dot(tok_rows.T, up_back, preferred_element_type=jnp.float32),
                      totals[2] + jnp.dot(cot_rows.T, hidden, preferred_element_type=jnp.float32))
        return new_totals, input_rows

    zeros = jnp.zeros((D, FF), jnp.float32)
    totals, input_blocks = lax.scan(accumulate, (zeros, zeros, zeros), jnp.arange(N_REP, dtype=jnp.int32))
    grad_scale = float(TOKENS) ** -0.5
    return (input_blocks.reshape(TOKENS, D), totals[0] * grad_scale, totals[1] * grad_scale, totals[2] * grad_scale)
```

```python
import functools

import jax
import jax.numpy as jnp
from jax import lax
from jax.experimental import pallas as pl
from jax.experimental.pallas import tpu as pltpu
from jax.sharding import PartitionSpec as P

MESH = pl.DeviceIdType.MESH
F32 = jnp.float32
BF16 = jnp.bfloat16
NY = 4


def body(
    nz, scale, tok_hbm, cot_hbm, gw_hbm, uw_hbm, dw_hbm, ig_ref, gg_ref, ug_ref, dg_ref,
    tok, cot, tokt, cott, gw, uw, dw, gpre, upre, hid, gb, ub, part, xhalf, xfull,
    prod, peer, summed, ya, za, zb, yb,
    ld_sem, ag_s, ag_r, dd_s, dd_r, xs_s, xs_r, rs_s, rs_r,
):
    rep = lax.axis_index("rep")
    x = lax.axis_index("fs")
    t = lax.axis_index("tp")
    nx = 4
    rows = tok.shape[1]
    half = rows // 2
    ff = gw.shape[1]
    d = gw.shape[0]
    z = rep // NY
    y = lax.rem(rep, NY)
    nxt, prv, opp = lax.rem(x + 1, nx), lax.rem(x + nx - 1, nx), lax.rem(x + 2, nx)
    other = 1 - t
    sgn = 1 - 2 * t

    def along_y(step):
        return lax.rem(y + NY + step, NY)

    def along_z(step):
        return lax.rem(z + nz + step, nz)

    def dev_y(step):
        return {"rep": z * NY + along_y(step)}

    def dev_z(step):
        return {"rep": along_z(step) * NY + y}

    loads = [
        pltpu.make_async_copy(src, dst, ld_sem.at[k])
        for k, (src, dst) in enumerate(
            [(tok_hbm, tok.at[x]), (gw_hbm, gw), (uw_hbm, uw), (cot_hbm, cot.at[x]), (dw_hbm, dw)]
        )
    ]
    for load in loads:
        load.start()

    barrier = pltpu.get_barrier_semaphore()
    peers = [{"fs": nxt}, {"fs": prv}, {"tp": other}, dev_y(1), dev_y(-1), dev_z(1), dev_z(-1)]
    for who in peers:
        pl.semaphore_signal(barrier, inc=1, device_id=who, device_id_type=MESH)
    pl.semaphore_wait(barrier, len(peers))

    def remote(src, dst, s, r, who):
        return pltpu.make_async_remote_copy(
            src_ref=src, dst_ref=dst, send_sem=s, recv_sem=r, device_id=who, device_id_type=MESH
        )

    bufs = (tok, cot)
    to = ({"fs": nxt}, {"fs": prv})
    came = (prv, nxt)

    def gather(a, way, k, slot, h):
        ref = bufs[a].at[slot, pl.ds(h * half, half), :]
        return remote(ref, ref, ag_s.at[a, way, k], ag_r.at[a, way, k], to[way])

    def gather_out(a):
        for k in range(2):
            for way in range(2):
                gather(a, way, k, x, k if way == 0 else 1 - k).start()

    def gather_in(a, way, k):
        if k == 2:
            gather(a, way, 2, opp, way).wait_recv()
        else:
            gather(a, way, k, came[way], k if way == 0 else 1 - k).wait_recv()

    def pass_on(a):
        for way in range(2):
            gather_in(a, way, 0)
            gather(a, way, 2, came[way], way).start()

    nt = 256

    def turned(src, dst, slot):
        at = pl.ds(pl.multiple_of(slot * rows, rows), rows)

        def one(i, _):
            cols = pl.ds(pl.multiple_of(i * nt, nt), nt)
            dst[cols, at] = src[slot, :, cols].T
            return 0

        lax.fori_loop(0, d // nt, one, 0)

    def forward(slot):
        def one(i, _):
            cols = pl.ds(pl.multiple_of(i * nt, nt), nt)
            g = jnp.dot(tok[slot], gw[:, cols], preferred_element_type=F32)
            u = jnp.dot(tok[slot], uw[:, cols], preferred_element_type=F32)
            gpre[slot, :, cols] = g
            upre[slot, :, cols] = u
            hid[slot, :, cols] = (g * jax.nn.sigmoid(g) * u).astype(BF16)
            return 0

        lax.fori_loop(0, ff // nt, one, 0)
        turned(tok, tokt, slot)

    def backward(slot):
        def one(i, _):
            cols = pl.ds(pl.multiple_of(i * nt, nt), nt)
            h = jnp.dot(cot[slot], dw[:, cols], preferred_element_type=F32)
            g = gpre[slot, :, cols]
            sig = jax.nn.sigmoid(g)
            gb[slot, :, cols] = (h * upre[slot, :, cols] * sig * (1.0 + g * (1.0 - sig))).astype(BF16)
            ub[slot, :, cols] = (h * (g * sig)).astype(BF16)
            return 0

        lax.fori_loop(0, ff // nt, one, 0)
        turned(cot, cott, slot)

    def input_part(slot):
        across = (((1,), (1,)), ((), ()))

        def one(i, _):
            cols = pl.ds(pl.multiple_of(i * nt, nt), nt)
            p = lax.dot_general(gb[slot], gw[cols, :], across, preferred_element_type=F32)
            p += lax.dot_general(ub[slot], uw[cols, :], across, preferred_element_type=F32)
            part[slot, :, cols] = p.astype(BF16)
            return 0

        lax.fori_loop(0, d // nt, one, 0)

    def x_first(way):
        return remote(
            part.at[opp, pl.ds(way * half, half), :], xhalf.at[way], xs_s.at[way], xs_r.at[way], to[way]
        )

    def x_second(way):
        return remote(part.at[(nxt, prv)[way]], xfull.at[way], xs_s.at[2 + way], xs_r.at[2 + way], to[way])

    def x_start():
        for way in range(2):
            x_first(way).start()

    def x_forward():
        for way in range(2):
            x_first(way).wait_recv()
            slot = (nxt, prv)[way]
            for i in range(half // 16):
                at = pl.ds(way * half + i * 16, 16)
                got = xhalf[way, pl.ds(i * 16, 16), :].astype(F32)
                part[slot, at, :] = (part[slot, at, :].astype(F32) + got).astype(BF16)
            x_second(way).start()

    def x_finish():
        for way in range(2):
            x_second(way).wait_recv()

        def one(i, _):
            at = pl.ds(pl.multiple_of(i * 16, 16), 16)
            total = part[x, at, :].astype(F32) + xfull[0, at, :].astype(F32) + xfull[1, at, :].astype(F32)
            ig_ref[at, :] = total.astype(BF16)
            return 0

        lax.fori_loop(0, rows // 16, one, 0)

    def pair(k, i):
        return remote(prod.at[k, i, :, other], peer.at[k, i], dd_s.at[k, i], dd_r.at[k, i], {"tp": other})

    dt = NY * 2 * 32

    def weight_sums(k, left, right):
        def one(i, _):
            lines = pl.ds(pl.multiple_of(i * dt, dt), dt)
            for j in range(ff // nt):
                cols = pl.ds(j * nt, nt)
                acc = jnp.dot(left[lines, 0:rows], right[0, :, cols], preferred_element_type=F32)
                for s in range(1, nx):
                    acc += jnp.dot(
                        left[lines, s * rows : (s + 1) * rows], right[s, :, cols], preferred_element_type=F32
                    )
                prod[k, i, :, :, :, cols] = acc.astype(BF16).reshape(NY, 2, 32, nt)
            pair(k, i).start()
            return 0

        lax.fori_loop(0, nz, one, 0)

    fa = ff // 2

    def pair_sum(k):
        def one(i, _):
            pair(k, i).wait_recv()
            for j in range(NY):
                both = prod[k, i, j, t].astype(F32) + peer[k, i, j].astype(F32)
                both = both.astype(BF16)
                summed[k, 0, i, j] = both[:, :fa]
                summed[k, 1, i, j] = both[:, fa:]
            return 0

        lax.fori_loop(0, nz, one, 0)

    ly, lz = (NY // 2, (NY - 1) // 2), (nz // 2, (nz - 1) // 2)
    per = sum(ly) + sum(lz)

    def chain_copy(k, half_no, axis, way, step):
        n_first = (ly, lz)[axis][0]
        m = step if way == 0 else n_first + step
        go = sgn if way == 0 else -sgn
        dist = ((ly, lz)[axis][way] - step) * go
        if half_no == 0:
            if axis == 0:
                src, dst = summed.at[k, 0, :, along_y(dist)], ya.at[k, m]
            else:
                src, dst = summed.at[k, 0, along_z(dist), y], za.at[k, m]
        else:
            if axis == 1:
                src, dst = summed.at[k, 1, along_z(dist)], zb.at[k, m]
            else:
                src, dst = summed.at[k, 1, z, along_y(dist)], yb.at[k, m]
        who = dev_y(go) if axis == 0 else dev_z(go)
        n = m if axis == (0 if half_no == 0 else 1) else (sum(ly) if half_no == 0 else sum(lz)) + m
        return remote(src, dst, rs_s.at[k, half_no, n], rs_r.at[k, half_no, n], who)

    def add_block(k, half_no, axis, step_to, ms):
        if half_no == 0 and axis == 0:
            at = along_y(step_to)

            def one(i, _):
                v = summed[k, 0, i, at].astype(F32)
                for m in ms:
                    v += ya[k, m, i].astype(F32)
                summed[k, 0, i, at] = v.astype(BF16)
                return 0

            lax.fori_loop(0, nz, one, 0)
        elif half_no == 0:
            at = along_z(step_to)
            v = summed[k, 0, at, y].astype(F32)
            for m in ms:
                v += za[k, m].astype(F32)
            summed[k, 0, at, y] = v.astype(BF16)
        elif axis == 1:
            at = along_z(step_to)

            def one(i, _):
                v = summed[k, 1, at, i].astype(F32)
                for m in ms:
                    v += zb[k, m, i].astype(F32)
                summed[k, 1, at, i] = v.astype(BF16)
                return 0

            lax.fori_loop(0, NY, one, 0)
        else:
            at = along_y(step_to)
            v = summed[k, 1, z, at].astype(F32)
            for m in ms:
                v += yb[k, m].astype(F32)
            summed[k, 1, z, at] = v.astype(BF16)

    outs = (dg_ref, gg_ref, ug_ref)

    def chain_step(k, half_no, axis, step):
        lens = (ly, lz)[axis]
        for way in range(2):
            if step >= lens[way]:
                continue
            if step > 0:
                chain_copy(k, half_no, axis, way, step - 1).wait_recv()
                go = sgn if way == 0 else -sgn
                m = step - 1 if way == 0 else lens[0] + step - 1
                add_block(k, half_no, axis, (lens[way] - step) * go, [m])
            chain_copy(k, half_no, axis, way, step).start()

    def chain_end(k, half_no, axis, last):
        lens = (ly, lz)[axis]
        ms = []
        for way in range(2):
            if lens[way]:
                chain_copy(k, half_no, axis, way, lens[way] - 1).wait_recv()
                ms.append(lens[way] - 1 if way == 0 else lens[0] + lens[1] - 1)
        if not last:
            add_block(k, half_no, axis, 0, ms)
            return
        v = summed[k, half_no, z, y].astype(F32)
        for m in ms:
            v += (za if half_no == 0 else yb)[k, m].astype(F32)
        outs[k][:, half_no * fa : (half_no + 1) * fa] = v * scale

    def stage(k, half_no, n):
        first, second = (0, 1) if half_no == 0 else (1, 0)
        n1, n2 = (ly, lz)[first][0], (ly, lz)[second][0]
        if n < n1:
            chain_step(k, half_no, first, n)
        elif n == n1:
            chain_end(k, half_no, first, False)
            chain_step(k, half_no, second, 0)
        elif n < n1 + n2:
            chain_step(k, half_no, second, n - n1)
        elif n == n1 + n2:
            chain_end(k, half_no, second, True)

    loads[0].wait()
    gather_out(0)
    loads[1].wait()
    loads[2].wait()
    forward(x)
    pass_on(0)
    loads[3].wait()
    gather_out(1)
    loads[4].wait()
    backward(x)
    input_part(x)
    gather_in(0, 0, 1)
    forward(prv)
    gather_in(0, 1, 1)
    forward(nxt)
    gather_in(0, 0, 2)
    gather_in(0, 1, 2)
    forward(opp)
    pass_on(1)
    gather_in(1, 0, 1)
    backward(prv)
    gather_in(1, 1, 1)
    backward(nxt)
    input_part(prv)
    input_part(nxt)
    gather_in(1, 0, 2)
    gather_in(1, 1, 2)
    backward(opp)
    weight_sums(0, cott, hid)
    weight_sums(1, tokt, gb)
    pair_sum(0)
    stage(0, 0, 0)
    stage(0, 1, 0)
    weight_sums(2, tokt, ub)
    pair_sum(1)
    stage(1, 0, 0)
    stage(1, 1, 0)
    input_part(opp)
    x_start()
    pair_sum(2)
    stage(2, 0, 0)
    stage(2, 1, 0)
    n_stages = ly[0] + lz[0] + 1
    for n in range(1, n_stages):
        for k in range(3):
            stage(k, 1, n)
            stage(k, 0, n)
        if n == 1:
            x_forward()
        if n == 4:
            x_finish()

    for a in range(2):
        for way in range(2):
            for k in range(2):
                gather(a, way, k, x, k if way == 0 else 1 - k).wait_send()
            gather(a, way, 2, came[way], way).wait_send()
    for way in range(2):
        x_first(way).wait_send()
        x_second(way).wait_send()

    def drain(i, _):
        for k in range(3):
            pair(k, i).wait_send()
        return 0

    lax.fori_loop(0, nz, drain, 0)
    for k in range(3):
        for half_no in range(2):
            for axis in range(2):
                for way in range(2):
                    for step in range((ly, lz)[axis][way]):
                        chain_copy(k, half_no, axis, way, step).wait_send()


def solution(mesh):
    n_rep = mesh.shape["rep"]
    nz = n_rep // NY
    nx = mesh.shape["fs"]
    cores = mesh.shape["tp"]

    def on_device(tokens, cotangent, gate_weight, up_weight, down_weight_t):
        rows, d = tokens.shape
        ff = gate_weight.shape[1]
        scale = float(rows * n_rep * nx * cores) ** (-0.5)
        lines = d // (n_rep * cores)
        fa = ff // 2
        ny_msgs, nz_msgs = NY - 1, nz - 1
        grad = jax.ShapeDtypeStruct((lines, ff), F32)
        vmem = pl.BlockSpec(memory_space=pltpu.VMEM)
        dma = pltpu.SemaphoreType.DMA
        return pl.pallas_call(
            functools.partial(body, nz, scale),
            out_shape=(jax.ShapeDtypeStruct((rows, d), BF16), grad, grad, grad),
            in_specs=[pl.BlockSpec(memory_space=pl.ANY)] * 5,
            out_specs=(vmem,) * 4,
            scratch_shapes=[
                pltpu.VMEM((nx, rows, d), BF16),
                pltpu.VMEM((nx, rows, d), BF16),
                pltpu.VMEM((d, nx * rows), BF16),
                pltpu.VMEM((d, nx * rows), BF16),
                pltpu.VMEM((d, ff), BF16),
                pltpu.VMEM((d, ff), BF16),
                pltpu.VMEM((d, ff), BF16),
                pltpu.VMEM((nx, rows, ff), F32),
                pltpu.VMEM((nx, rows, ff), F32),
                pltpu.VMEM((nx, rows, ff), BF16),
                pltpu.VMEM((nx, rows, ff), BF16),
                pltpu.VMEM((nx, rows, ff), BF16),
                pltpu.VMEM((nx, rows, d), BF16),
                pltpu.VMEM((2, rows // 2, d), BF16),
                pltpu.VMEM((2, rows, d), BF16),
                pltpu.VMEM((3, nz, NY, cores, lines, ff), BF16),
                pltpu.VMEM((3, nz, NY, lines, ff), BF16),
                pltpu.VMEM((3, 2, nz, NY, lines, fa), BF16),
                pltpu.VMEM((3, ny_msgs, nz, lines, fa), BF16),
                pltpu.VMEM((3, nz_msgs, lines, fa), BF16),
                pltpu.VMEM((3, nz_msgs, NY, lines, fa), BF16),
                pltpu.VMEM((3, ny_msgs, lines, fa), BF16),
                dma((5,)),
                dma((2, 2, 3)),
                dma((2, 2, 3)),
                dma((3, nz)),
                dma((3, nz)),
                dma((4,)),
                dma((4,)),
                dma((3, 2, ny_msgs + nz_msgs)),
                dma((3, 2, ny_msgs + nz_msgs)),
            ],
            compiler_params=pltpu.CompilerParams(
                collective_id=0, has_side_effects=True, vmem_limit_bytes=64 * 1024 * 1024 - 128 * 1024
            ),
        )(tokens, cotangent, gate_weight, up_weight, down_weight_t)

    return jax.shard_map(
        on_device,
        mesh=mesh,
        in_specs=(
            P(("rep", "fs", "tp"), None),
            P(("rep", "fs", "tp"), None),
            P(None, "fs"),
            P(None, "fs"),
            P(None, "fs"),
        ),
        out_specs=(
            P(("rep", "fs", "tp"), None),
            P(("rep", "tp"), "fs"),
            P(("rep", "tp"), "fs"),
            P(("rep", "tp"), "fs"),
        ),
        check_vma=False,
    )
```

```python
import functools

import jax
import jax.numpy as jnp
from jax import lax
from jax.experimental import pallas as pl
from jax.experimental.pallas import tpu as pltpu
from jax.sharding import PartitionSpec as P

MESH = pl.DeviceIdType.MESH
F32 = jnp.float32
BF16 = jnp.bfloat16
NY = 4


def body(
    nz, scale, tok_hbm, cot_hbm, gw_hbm, uw_hbm, dw_hbm, ig_ref, gg_ref, ug_ref, dg_ref,
    tok, cot, tokt, cott, gw, uw, dw, gwt, uwt, gpre, upre, hid, gb, ub, part, xhalf, xfull,
    prod, peer, summed, ya, za, zb, yb,
    ld_sem, ag_s, ag_r, dd_s, dd_r, xs_s, xs_r, rs_s, rs_r,
):
    rep = lax.axis_index("rep")
    x = lax.axis_index("fs")
    t = lax.axis_index("tp")
    nx = 4
    rows = tok.shape[1]
    half = rows // 2
    ff = gw.shape[1]
    d = gw.shape[0]
    z = rep // NY
    y = lax.rem(rep, NY)
    nxt, prv, opp = lax.rem(x + 1, nx), lax.rem(x + nx - 1, nx), lax.rem(x + 2, nx)
    other = 1 - t
    sgn = 1 - 2 * t

    def along_y(step):
        return lax.rem(y + NY + step, NY)

    def along_z(step):
        return lax.rem(z + nz + step, nz)

    def dev_y(step):
        return {"rep": z * NY + along_y(step)}

    def dev_z(step):
        return {"rep": along_z(step) * NY + y}

    loads = [
        pltpu.make_async_copy(src, dst, ld_sem.at[k])
        for k, (src, dst) in enumerate(
            [(tok_hbm, tok.at[x]), (gw_hbm, gw), (uw_hbm, uw), (cot_hbm, cot.at[x]), (dw_hbm, dw)]
        )
    ]
    for load in loads:
        load.start()

    barrier = pltpu.get_barrier_semaphore()
    peers = [{"fs": nxt}, {"fs": prv}, {"tp": other}, dev_y(1), dev_y(-1), dev_z(1), dev_z(-1)]
    for who in peers:
        pl.semaphore_signal(barrier, inc=1, device_id=who, device_id_type=MESH)
    pl.semaphore_wait(barrier, len(peers))

    def remote(src, dst, s, r, who):
        return pltpu.make_async_remote_copy(
            src_ref=src, dst_ref=dst, send_sem=s, recv_sem=r, device_id=who, device_id_type=MESH
        )

    bufs = (tok, cot)
    to = ({"fs": nxt}, {"fs": prv})
    came = (prv, nxt)

    def gather(a, way, k, slot, h):
        ref = bufs[a].at[slot, pl.ds(h * half, half), :]
        return remote(ref, ref, ag_s.at[a, way, k], ag_r.at[a, way, k], to[way])

    def gather_out(a):
        for k in range(2):
            for way in range(2):
                gather(a, way, k, x, k if way == 0 else 1 - k).start()

    def gather_in(a, way, k):
        if k == 2:
            gather(a, way, 2, opp, way).wait_recv()
        else:
            gather(a, way, k, came[way], k if way == 0 else 1 - k).wait_recv()

    def pass_on(a):
        for way in range(2):
            gather_in(a, way, 0)
            gather(a, way, 2, came[way], way).start()

    nt = 256

    def rows_of(slot):
        return pl.ds(pl.multiple_of(slot * rows, rows), rows)

    def turned(src, dst, slot):
        dst[:, rows_of(slot)] = src[slot].T

    def turn_weights():
        def one(i, _):
            lines = pl.ds(pl.multiple_of(i * nt, nt), nt)
            gwt[:, lines] = gw[lines, :].T
            uwt[:, lines] = uw[lines, :].T
            return 0

        lax.fori_loop(0, d // nt, one, 0)

    def forward(slot):
        at = rows_of(slot)

        def one(i):
            cols = pl.ds(i * nt, nt)
            g = jnp.dot(tok[slot], gw[:, cols], preferred_element_type=F32)
            u = jnp.dot(tok[slot], uw[:, cols], preferred_element_type=F32)
            gpre[slot, :, cols] = g
            upre[slot, :, cols] = u
            hid[at, cols] = (g * jax.nn.sigmoid(g) * u).astype(BF16)

        for i in range(ff // nt):
            one(i)
        turned(tok, tokt, slot)

    def backward(slot):
        at = rows_of(slot)

        def one(i):
            cols = pl.ds(i * nt, nt)
            h = jnp.dot(cot[slot], dw[:, cols], preferred_element_type=F32)
            g = gpre[slot, :, cols]
            sig = jax.nn.sigmoid(g)
            gb[at, cols] = (h * upre[slot, :, cols] * sig * (1.0 + g * (1.0 - sig))).astype(BF16)
            ub[at, cols] = (h * (g * sig)).astype(BF16)

        for i in range(ff // nt):
            one(i)

    def input_part(slot):
        at = rows_of(slot)
        for i in range(d // nt):
            cols = pl.ds(i * nt, nt)
            p = jnp.dot(gb[at, :], gwt[:, cols], preferred_element_type=F32)
            p += jnp.dot(ub[at, :], uwt[:, cols], preferred_element_type=F32)
            part[slot, :, cols] = p.astype(BF16)

    def x_first(way):
        return remote(
            part.at[opp, pl.ds(way * half, half), :], xhalf.at[way], xs_s.at[way], xs_r.at[way], to[way]
        )

    def x_second(way):
        return remote(part.at[(nxt, prv)[way]], xfull.at[way], xs_s.at[2 + way], xs_r.at[2 + way], to[way])

    def x_start():
        for way in range(2):
            x_first(way).start()

    def x_forward():
        for way in range(2):
            x_first(way).wait_recv()
            slot = (nxt, prv)[way]
            for i in range(half // 16):
                at = pl.ds(way * half + i * 16, 16)
                got = xhalf[way, pl.ds(i * 16, 16), :].astype(F32)
                part[slot, at, :] = (part[slot, at, :].astype(F32) + got).astype(BF16)
            x_second(way).start()

    def x_finish():
        for way in range(2):
            x_second(way).wait_recv()

        def one(i, _):
            at = pl.ds(pl.multiple_of(i * 16, 16), 16)
            total = part[x, at, :].astype(F32) + xfull[0, at, :].astype(F32) + xfull[1, at, :].astype(F32)
            ig_ref[at, :] = total.astype(BF16)
            return 0

        lax.fori_loop(0, rows // 16, one, 0)

    def pair(k, i):
        zs = pl.ds(i * zt, zt)
        return remote(prod.at[k, zs, :, other], peer.at[k, zs], dd_s.at[k, i], dd_r.at[k, i], {"tp": other})

    zt = 2
    dt = zt * NY * 2 * 32

    def weight_sums(k, left, right, steps):
        for i in steps:
            lines = pl.ds(i * dt, dt)
            for j in range(ff // nt):
                cols = pl.ds(j * nt, nt)
                acc = jnp.dot(left[lines, :], right[:, cols], preferred_element_type=F32)
                prod[k, i * zt : (i + 1) * zt, :, :, :, cols] = acc.astype(BF16).reshape(zt, NY, 2, 32, nt)
            pair(k, i).start()

    fa = ff // 2

    def pair_sum(k):
        for i in range(nz // zt):
            pair(k, i).wait_recv()

        def one(i, _):
            for j in range(NY):
                both = prod[k, i, j, t].astype(F32) + peer[k, i, j].astype(F32)
                both = both.astype(BF16)
                summed[k, 0, i, j] = both[:, :fa]
                summed[k, 1, i, j] = both[:, fa:]
            return 0

        lax.fori_loop(0, nz, one, 0)

    ly, lz = (NY // 2, (NY - 1) // 2), (nz // 2, (nz - 1) // 2)
    per = sum(ly) + sum(lz)

    def chain_copy(k, half_no, axis, way, step):
        n_first = (ly, lz)[axis][0]
        m = step if way == 0 else n_first + step
        go = sgn if way == 0 else -sgn
        dist = ((ly, lz)[axis][way] - step) * go
        if half_no == 0:
            if axis == 0:
                src, dst = summed.at[k, 0, :, along_y(dist)], ya.at[k, m]
            else:
                src, dst = summed.at[k, 0, along_z(dist), y], za.at[k, m]
        else:
            if axis == 1:
                src, dst = summed.at[k, 1, along_z(dist)], zb.at[k, m]
            else:
                src, dst = summed.at[k, 1, z, along_y(dist)], yb.at[k, m]
        who = dev_y(go) if axis == 0 else dev_z(go)
        n = m if axis == (0 if half_no == 0 else 1) else (sum(ly) if half_no == 0 else sum(lz)) + m
        return remote(src, dst, rs_s.at[k, half_no, n], rs_r.at[k, half_no, n], who)

    def add_block(k, half_no, axis, step_to, ms):
        if half_no == 0 and axis == 0:
            at = along_y(step_to)

            def one(i, _):
                v = summed[k, 0, i, at].astype(F32)
                for m in ms:
                    v += ya[k, m, i].astype(F32)
                summed[k, 0, i, at] = v.astype(BF16)
                return 0

            lax.fori_loop(0, nz, one, 0)
        elif half_no == 0:
            at = along_z(step_to)
            v = summed[k, 0, at, y].astype(F32)
            for m in ms:
                v += za[k, m].astype(F32)
            summed[k, 0, at, y] = v.astype(BF16)
        elif axis == 1:
            at = along_z(step_to)

            def one(i, _):
                v = summed[k, 1, at, i].astype(F32)
                for m in ms:
                    v += zb[k, m, i].astype(F32)
                summed[k, 1, at, i] = v.astype(BF16)
                return 0

            lax.fori_loop(0, NY, one, 0)
        else:
            at = along_y(step_to)
            v = summed[k, 1, z, at].astype(F32)
            for m in ms:
                v += yb[k, m].astype(F32)
            summed[k, 1, z, at] = v.astype(BF16)

    outs = (dg_ref, gg_ref, ug_ref)

    def chain_step(k, half_no, axis, step):
        lens = (ly, lz)[axis]
        for way in range(2):
            if step >= lens[way]:
                continue
            if step > 0:
                chain_copy(k, half_no, axis, way, step - 1).wait_recv()
                go = sgn if way == 0 else -sgn
                m = step - 1 if way == 0 else lens[0] + step - 1
                add_block(k, half_no, axis, (lens[way] - step) * go, [m])
            chain_copy(k, half_no, axis, way, step).start()

    def chain_end(k, half_no, axis, last):
        lens = (ly, lz)[axis]
        ms = []
        for way in range(2):
            if lens[way]:
                chain_copy(k, half_no, axis, way, lens[way] - 1).wait_recv()
                ms.append(lens[way] - 1 if way == 0 else lens[0] + lens[1] - 1)
        if not last:
            add_block(k, half_no, axis, 0, ms)
            return
        v = summed[k, half_no, z, y].astype(F32)
        for m in ms:
            v += (za if half_no == 0 else yb)[k, m].astype(F32)
        outs[k][:, half_no * fa : (half_no + 1) * fa] = v * scale

    def stage(k, half_no, n):
        first, second = (0, 1) if half_no == 0 else (1, 0)
        n1, n2 = (ly, lz)[first][0], (ly, lz)[second][0]
        if n < n1:
            chain_step(k, half_no, first, n)
        elif n == n1:
            chain_end(k, half_no, first, False)
            chain_step(k, half_no, second, 0)
        elif n < n1 + n2:
            chain_step(k, half_no, second, n - n1)
        elif n == n1 + n2:
            chain_end(k, half_no, second, True)

    early, late = range(nz // zt // 2), range(nz // zt // 2, nz // zt)
    loads[0].wait()
    gather_out(0)
    loads[1].wait()
    loads[2].wait()
    forward(x)
    turn_weights()
    pass_on(0)
    loads[3].wait()
    gather_out(1)
    loads[4].wait()
    backward(x)
    turned(cot, cott, x)
    input_part(x)
    gather_in(0, 0, 1)
    forward(prv)
    gather_in(0, 1, 1)
    forward(nxt)
    gather_in(0, 0, 2)
    gather_in(0, 1, 2)
    forward(opp)
    pass_on(1)
    gather_in(1, 0, 1)
    backward(prv)
    turned(cot, cott, prv)
    gather_in(1, 1, 1)
    backward(nxt)
    turned(cot, cott, nxt)
    gather_in(1, 0, 2)
    gather_in(1, 1, 2)
    turned(cot, cott, opp)
    weight_sums(0, cott, hid, early)
    weight_sums(0, cott, hid, late)
    backward(opp)
    weight_sums(1, tokt, gb, early)
    pair_sum(0)
    stage(0, 0, 0)
    stage(0, 1, 0)
    weight_sums(1, tokt, gb, late)
    weight_sums(2, tokt, ub, early)
    pair_sum(1)
    stage(1, 0, 0)
    stage(1, 1, 0)
    weight_sums(2, tokt, ub, late)
    input_part(opp)
    x_start()
    pair_sum(2)
    stage(2, 0, 0)
    stage(2, 1, 0)
    input_part(prv)
    input_part(nxt)
    n_stages = ly[0] + lz[0] + 1
    for n in range(1, n_stages):
        for k in range(3):
            stage(k, 1, n)
            stage(k, 0, n)
        if n == 1:
            x_forward()
        if n == 4:
            x_finish()

    for a in range(2):
        for way in range(2):
            for k in range(2):
                gather(a, way, k, x, k if way == 0 else 1 - k).wait_send()
            gather(a, way, 2, came[way], way).wait_send()
    for way in range(2):
        x_first(way).wait_send()
        x_second(way).wait_send()

    for k in range(3):
        for i in range(nz // zt):
            pair(k, i).wait_send()
    for k in range(3):
        for half_no in range(2):
            for axis in range(2):
                for way in range(2):
                    for step in range((ly, lz)[axis][way]):
                        chain_copy(k, half_no, axis, way, step).wait_send()


def written(*refs):
    n = (len(refs) - 1) // 2
    copies = [pltpu.make_async_copy(refs[k], refs[n + k], refs[-1].at[k]) for k in range(n)]
    for copy in copies:
        copy.start()
    for copy in copies:
        copy.wait()


def solution(mesh):
    n_rep = mesh.shape["rep"]
    nz = n_rep // NY
    nx = mesh.shape["fs"]
    cores = mesh.shape["tp"]

    def on_device(tokens, cotangent, gate_weight, up_weight, down_weight_t):
        rows, d = tokens.shape
        ff = gate_weight.shape[1]
        scale = float(rows * n_rep * nx * cores) ** (-0.5)
        lines = d // (n_rep * cores)
        fa = ff // 2
        ny_msgs, nz_msgs = NY - 1, nz - 1
        shapes = (((rows, d), BF16),) + (((lines, ff), F32),) * 3
        vmem = pl.BlockSpec(memory_space=pltpu.VMEM)
        dma = pltpu.SemaphoreType.DMA
        results = pl.pallas_call(
            functools.partial(body, nz, scale),
            out_shape=tuple(pltpu.VMEM(*s) for s in shapes),
            in_specs=[pl.BlockSpec(memory_space=pl.ANY)] * 5,
            out_specs=(vmem,) * 4,
            scratch_shapes=[
                pltpu.VMEM((nx, rows, d), BF16),
                pltpu.VMEM((nx, rows, d), BF16),
                pltpu.VMEM((d, nx * rows), BF16),
                pltpu.VMEM((d, nx * rows), BF16),
                pltpu.VMEM((d, ff), BF16),
                pltpu.VMEM((d, ff), BF16),
                pltpu.VMEM((d, ff), BF16),
                pltpu.VMEM((ff, d), BF16),
                pltpu.VMEM((ff, d), BF16),
                pltpu.VMEM((nx, rows, ff), F32),
                pltpu.VMEM((nx, rows, ff), F32),
                pltpu.VMEM((nx * rows, ff), BF16),
                pltpu.VMEM((nx * rows, ff), BF16),
                pltpu.VMEM((nx * rows, ff), BF16),
                pltpu.VMEM((nx, rows, d), BF16),
                pltpu.VMEM((2, rows // 2, d), BF16),
                pltpu.VMEM((2, rows, d), BF16),
                pltpu.VMEM((3, nz, NY, cores, lines, ff), BF16),
                pltpu.VMEM((3, nz, NY, lines, ff), BF16),
                pltpu.VMEM((3, 2, nz, NY, lines, fa), BF16),
                pltpu.VMEM((3, ny_msgs, nz, lines, fa), BF16),
                pltpu.VMEM((3, nz_msgs, lines, fa), BF16),
                pltpu.VMEM((3, nz_msgs, NY, lines, fa), BF16),
                pltpu.VMEM((3, ny_msgs, lines, fa), BF16),
                dma((5,)),
                dma((2, 2, 3)),
                dma((2, 2, 3)),
                dma((3, nz // 2)),
                dma((3, nz // 2)),
                dma((4,)),
                dma((4,)),
                dma((3, 2, ny_msgs + nz_msgs)),
                dma((3, 2, ny_msgs + nz_msgs)),
            ],
            compiler_params=pltpu.CompilerParams(
                collective_id=0, has_side_effects=True, vmem_limit_bytes=60 * 1024 * 1024
            ),
        )(tokens, cotangent, gate_weight, up_weight, down_weight_t)
        return pl.pallas_call(
            written,
            out_shape=tuple(jax.ShapeDtypeStruct(*s) for s in shapes),
            in_specs=[vmem] * 4,
            out_specs=(pl.BlockSpec(memory_space=pltpu.HBM),) * 4,
            scratch_shapes=[dma((4,))],
        )(*[pltpu.with_memory_space_constraint(r, pltpu.VMEM) for r in results])

    return jax.shard_map(
        on_device,
        mesh=mesh,
        in_specs=(
            P(("rep", "fs", "tp"), None),
            P(("rep", "fs", "tp"), None),
            P(None, "fs"),
            P(None, "fs"),
            P(None, "fs"),
        ),
        out_specs=(
            P(("rep", "fs", "tp"), None),
            P(("rep", "tp"), "fs"),
            P(("rep", "tp"), "fs"),
            P(("rep", "tp"), "fs"),
        ),
        check_vma=False,
    )
```

```python
import functools

import jax
import jax.numpy as jnp
from jax import lax
from jax.experimental import pallas as pl
from jax.experimental.pallas import tpu as pltpu
from jax.sharding import PartitionSpec as P

MESH = pl.DeviceIdType.MESH
F32 = jnp.float32
BF16 = jnp.bfloat16
NY = 4
WIDTH_A = (384, 384, 512)


def body(
    nz, scale, tok_hbm, cot_hbm, gw_hbm, uw_hbm, dw_hbm, ig_ref, gg_ref, ug_ref, dg_ref,
    tok, cot, tokt, cott, gw, uw, dw, gwt, uwt, gpre, upre, hpre, hid, gb, ub, part, xhalf, xfull,
    prod, peer, *rest,
):
    sa, sb, ya, za, zb, yb = (rest[3 * i : 3 * i + 3] for i in range(6))
    ld_sem, ag_s, ag_r, dd_s, dd_r, xs_s, xs_r, rs_s, rs_r = rest[18:]
    rep = lax.axis_index("rep")
    x = lax.axis_index("fs")
    t = lax.axis_index("tp")
    nx = 4
    rows = tok.shape[1]
    half = rows // 2
    d, ff = gw.shape
    hd = d // 2
    zw = d // nz
    hz = nz // 2
    z = rep // NY
    y = lax.rem(rep, NY)
    nxt, prv, opp = lax.rem(x + 1, nx), lax.rem(x + nx - 1, nx), lax.rem(x + 2, nx)
    other = 1 - t
    sgn = 1 - 2 * t

    def along_y(step):
        return lax.rem(y + NY + step, NY)

    def along_z(step):
        return lax.rem(z + nz + step, nz)

    def place(zi):
        return zi % 2 * hz + zi // 2 if isinstance(zi, int) else lax.rem(zi, 2) * hz + zi // 2

    def dev_y(step):
        return {"rep": z * NY + along_y(step)}

    def dev_z(step):
        return {"rep": along_z(step) * NY + y}

    def on_parity(e, yes, no=None):
        mine = lax.rem(z, 2) == e
        pl.when(mine)(yes)
        if no is not None:
            pl.when(jnp.logical_not(mine))(no)

    parts = [(tok_hbm, tok.at[x]), (gw_hbm, gw), (uw_hbm, uw)]
    for zi in range(nz):
        cols = pl.ds(zi * zw, zw)
        parts.append((cot_hbm.at[:, cols], cot.at[zi % 2, x, :, pl.ds(zi // 2 * zw, zw)]))
    for zi in range(nz):
        parts.append((dw_hbm.at[pl.ds(zi * zw, zw), :], dw.at[pl.ds(place(zi) * zw, zw), :]))
    loads = [pltpu.make_async_copy(src, dst, ld_sem.at[k]) for k, (src, dst) in enumerate(parts)]
    for load in loads:
        load.start()

    barrier = pltpu.get_barrier_semaphore()
    peers = [{"fs": nxt}, {"fs": prv}, {"tp": other}]
    peers += [dev_y(s) for s in (1, -1, 2)] + [dev_z(s) for s in (1, -1, 2, -2)]
    for who in peers:
        pl.semaphore_signal(barrier, inc=1, device_id=who, device_id_type=MESH)
    pl.semaphore_wait(barrier, len(peers))

    def remote(src, dst, s, r, who):
        return pltpu.make_async_remote_copy(
            src_ref=src, dst_ref=dst, send_sem=s, recv_sem=r, device_id=who, device_id_type=MESH
        )

    bufs = (tok, cot.at[0], cot.at[1])
    to = ({"fs": nxt}, {"fs": prv})
    came = (prv, nxt)

    def gather(a, way, k, slot, h):
        ref = bufs[a].at[slot, pl.ds(h * half, half), :]
        return remote(ref, ref, ag_s.at[a, way, k], ag_r.at[a, way, k], to[way])

    def gather_out(a):
        for k in range(2):
            for way in range(2):
                gather(a, way, k, x, k if way == 0 else 1 - k).start()

    def gather_in(a, way, k):
        if k == 2:
            gather(a, way, 2, opp, way).wait_recv()
        else:
            gather(a, way, k, came[way], k if way == 0 else 1 - k).wait_recv()

    def pass_on(a):
        for way in range(2):
            gather_in(a, way, 0)
            gather(a, way, 2, came[way], way).start()

    nt = 256

    def rows_of(slot):
        return pl.ds(pl.multiple_of(slot * rows, rows), rows)

    def turned_cot(e, slot):
        cott[e * hd : (e + 1) * hd, rows_of(slot)] = cot[e, slot].T

    def turn_weights():
        def one(i, _):
            lines = pl.ds(pl.multiple_of(i * nt, nt), nt)
            gwt[:, lines] = gw[lines, :].T
            uwt[:, lines] = uw[lines, :].T
            return 0

        lax.fori_loop(0, d // nt, one, 0)

    def forward(slot):
        at = rows_of(slot)
        for i in range(ff // nt):
            cols = pl.ds(i * nt, nt)
            g = jnp.dot(tok[slot], gw[:, cols], preferred_element_type=F32)
            u = jnp.dot(tok[slot], uw[:, cols], preferred_element_type=F32)
            gpre[slot, :, cols] = g
            upre[slot, :, cols] = u
            hid[at, cols] = (g * jax.nn.sigmoid(g) * u).astype(BF16)
        for zi in range(nz):
            tokt[place(zi) * zw : (place(zi) + 1) * zw, at] = tok[slot, :, zi * zw : (zi + 1) * zw].T

    def hid_part(slot):
        for i in range(ff // nt):
            cols = pl.ds(i * nt, nt)
            hpre[slot, :, cols] = jnp.dot(cot[0, slot], dw[0:hd, cols], preferred_element_type=F32)

    def backward(slot):
        at = rows_of(slot)
        for i in range(ff // nt):
            cols = pl.ds(i * nt, nt)
            h = hpre[slot, :, cols] + jnp.dot(cot[1, slot], dw[hd:d, cols], preferred_element_type=F32)
            g = gpre[slot, :, cols]
            sig = jax.nn.sigmoid(g)
            gb[at, cols] = (h * upre[slot, :, cols] * sig * (1.0 + g * (1.0 - sig))).astype(BF16)
            ub[at, cols] = (h * (g * sig)).astype(BF16)

    def input_part(slot):
        at = rows_of(slot)
        for i in range(d // nt):
            cols = pl.ds(i * nt, nt)
            p = jnp.dot(gb[at, :], gwt[:, cols], preferred_element_type=F32)
            p += jnp.dot(ub[at, :], uwt[:, cols], preferred_element_type=F32)
            part[slot, :, cols] = p.astype(BF16)

    def x_first(way):
        return remote(
            part.at[opp, pl.ds(way * half, half), :], xhalf.at[way], xs_s.at[way], xs_r.at[way], to[way]
        )

    def x_second(way):
        return remote(part.at[(nxt, prv)[way]], xfull.at[way], xs_s.at[2 + way], xs_r.at[2 + way], to[way])

    def x_start():
        for way in range(2):
            x_first(way).start()

    def x_forward():
        for way in range(2):
            x_first(way).wait_recv()
            slot = (nxt, prv)[way]
            for i in range(half // 16):
                at = pl.ds(way * half + i * 16, 16)
                got = xhalf[way, pl.ds(i * 16, 16), :].astype(F32)
                part[slot, at, :] = (part[slot, at, :].astype(F32) + got).astype(BF16)
            x_second(way).start()

    def x_finish():
        for way in range(2):
            x_second(way).wait_recv()

        def one(i, _):
            at = pl.ds(pl.multiple_of(i * 16, 16), 16)
            total = part[x, at, :].astype(F32) + xfull[0, at, :].astype(F32) + xfull[1, at, :].astype(F32)
            ig_ref[at, :] = total.astype(BF16)
            return 0

        lax.fori_loop(0, rows // 16, one, 0)

    zt = 2

    def pair(k, i):
        at = pl.ds(i * zt, zt)
        return remote(prod.at[k, at, :, other], peer.at[k, at], dd_s.at[k, i], dd_r.at[k, i], {"tp": other})

    left, right, outs = (cott, tokt, tokt), (hid, gb, ub), (dg_ref, gg_ref, ug_ref)

    def weight_sums(k, e):
        for i in range(e * hz // zt, (e + 1) * hz // zt):
            lines = pl.ds(i * zt * zw, zt * zw)
            for j in range(ff // nt):
                cols = pl.ds(j * nt, nt)
                acc = jnp.dot(left[k][lines, :], right[k][:, cols], preferred_element_type=F32)
                prod[k, i * zt : (i + 1) * zt, :, :, :, cols] = acc.astype(BF16).reshape(zt, NY, 2, 32, nt)
            pair(k, i).start()

    def pair_sum(k, e):
        for i in range(e * hz // zt, (e + 1) * hz // zt):
            pair(k, i).wait_recv()
        wa = WIDTH_A[k]

        def one(i, _):
            for j in range(NY):
                both = prod[k, i, j, t].astype(F32) + peer[k, i, j].astype(F32)
                both = both.astype(BF16)
                sa[k][i, j] = both[:, :wa]
                sb[k][i, j] = both[:, wa:]
            return 0

        lax.fori_loop(e * hz, (e + 1) * hz, one, 0)

    ly, lz = (2, 1), (4, 3)

    def sems(k, e, h, n):
        u = (k * 2 + e) * 2 + h
        return rs_s.at[u, n], rs_r.at[u, n]

    def go(way):
        return sgn if way == 0 else -sgn

    def a_y(k, e, way, step):
        m = step if way == 0 else 2
        at = pl.ds(e * hz, hz)
        dest = along_y((ly[way] - step) * go(way))
        return remote(sa[k].at[at, dest], ya[k].at[m, at], *sems(k, e, 0, m), dev_y(go(way)))

    hops = {"a": (4, 2), "b": (3, 1), "c": (1, 1), "d": (2, 2), "e": (-3, -2), "f": (-2, -1), "g": (-1, -1)}

    def a_z(k, e, name):
        m = "abcdefg".index(name)
        owner, target = hops[name]
        src = sa[k].at[place(along_z(owner * sgn)), y]
        return remote(src, za[k].at[m], *sems(k, e, 0, 3 + m), dev_z(target * sgn))

    def b_z(k, e, way, step):
        m = step if way == 0 else lz[0] + step
        src = sb[k].at[place(along_z((lz[way] - step) * go(way)))]
        return remote(src, zb[k].at[m], *sems(k, e, 1, m), dev_z(go(way)))

    y_steps = (1, -1, 2)

    def b_y(k, e, m):
        src = sb[k].at[place(z), along_y(y_steps[m])]
        return remote(src, yb[k].at[m], *sems(k, e, 1, 7 + m), dev_y(y_steps[m]))

    def added(ref, at, arrived):
        v = ref[at].astype(F32)
        for got in arrived:
            v += got.astype(F32)
        return v

    def a_stage(k, e, n):
        names = "abcdefg"
        if n <= 1:
            for way in range(2):
                if n >= ly[way]:
                    continue
                if n == 1:
                    a_y(k, e, way, 0).wait_recv()
                    at = along_y((ly[way] - 1) * go(way))
                    for i in range(e * hz, (e + 1) * hz):
                        sa[k][i, at] = added(sa[k], (i, at), [ya[k][0, i]]).astype(BF16)
                a_y(k, e, way, n).start()
        elif n == 2:
            a_y(k, e, 0, 1).wait_recv()
            a_y(k, e, 1, 0).wait_recv()
            for i in range(e * hz, (e + 1) * hz):
                sa[k][i, y] = added(sa[k], (i, y), [ya[k][1, i], ya[k][2, i]]).astype(BF16)

            def yes():
                for name in "af":
                    a_z(k, e, name).start()

            def no():
                for name in "ecb":
                    a_z(k, e, name).start()

            on_parity(e, yes, no)
        elif n == 3:

            def relay(one, two, step, out):
                a_z(k, e, one).wait_recv()
                a_z(k, e, two).wait_recv()
                at = (place(along_z(step * sgn)), y)
                got = [za[k][names.index(one)], za[k][names.index(two)]]
                sa[k][at] = added(sa[k], at, got).astype(BF16)
                a_z(k, e, out).start()

            on_parity(e, lambda: relay("a", "b", 2, "d"), lambda: relay("e", "f", -1, "g"))
        else:

            def end():
                for name in "cdg":
                    a_z(k, e, name).wait_recv()
                v = added(sa[k], (place(z), y), [za[k][names.index(c)] for c in "cdg"])
                outs[k][:, : WIDTH_A[k]] = v * scale

            on_parity(e, end)

    def b_sum(k, at, ms):
        for j in range(NY):
            sb[k][at, j] = added(sb[k], (at, j), [zb[k][m, j] for m in ms]).astype(BF16)

    def b_stage(k, e, n):
        if n <= 3:

            def step(way):
                if n > 0:
                    b_z(k, e, way, n - 1).wait_recv()
                    m = n - 1 if way == 0 else lz[0] + n - 1
                    b_sum(k, place(along_z((lz[way] - n) * go(way))), [m])
                b_z(k, e, way, n).start()

            def steps(rest_of):
                def run():
                    for way in range(2):
                        if n < lz[way] and (lz[way] - n) % 2 == rest_of:
                            step(way)

                return run

            on_parity(e, steps(0), steps(1))
        elif n == 4:

            def turn():
                b_z(k, e, 0, 3).wait_recv()
                b_z(k, e, 1, 2).wait_recv()
                b_sum(k, place(z), [3, 6])
                for m in range(3):
                    b_y(k, e, m).start()

            on_parity(e, turn)
        else:

            def end():
                for m in range(3):
                    b_y(k, e, m).wait_recv()
                v = added(sb[k], (place(z), y), [yb[k][m] for m in range(3)])
                outs[k][:, WIDTH_A[k] :] = v * scale

            on_parity(e, end)

    def stage(k, e, h, n):
        (a_stage, b_stage)[h](k, e, n)

    loads[0].wait()
    gather_out(0)
    loads[1].wait()
    loads[2].wait()
    forward(x)
    turn_weights()
    pass_on(0)
    for load in loads[3 : 3 + nz]:
        load.wait()
    gather_out(1)
    for load in loads[3 + nz :]:
        load.wait()
    hid_part(x)
    turned_cot(0, x)
    backward(x)
    turned_cot(1, x)
    input_part(x)
    gather_in(0, 0, 1)
    forward(prv)
    gather_in(0, 1, 1)
    forward(nxt)
    gather_in(0, 0, 2)
    gather_in(0, 1, 2)
    forward(opp)
    pass_on(1)
    gather_out(2)
    gather_in(1, 0, 1)
    hid_part(prv)
    turned_cot(0, prv)
    gather_in(1, 1, 1)
    hid_part(nxt)
    turned_cot(0, nxt)
    gather_in(1, 0, 2)
    gather_in(1, 1, 2)
    turned_cot(0, opp)
    weight_sums(0, 0)
    hid_part(opp)
    pair_sum(0, 0)
    stage(0, 0, 1, 0)
    stage(0, 0, 0, 0)
    pass_on(2)
    gather_in(2, 0, 1)
    gather_in(2, 1, 1)
    backward(prv)
    stage(0, 0, 1, 1)
    backward(nxt)
    turned_cot(1, prv)
    turned_cot(1, nxt)
    stage(0, 0, 0, 1)
    gather_in(2, 0, 2)
    gather_in(2, 1, 2)
    turned_cot(1, opp)
    weight_sums(0, 1)
    stage(0, 0, 1, 2)
    backward(opp)
    weight_sums(1, 0)
    stage(0, 0, 0, 2)
    pair_sum(0, 1)
    stage(0, 1, 1, 0)
    stage(0, 1, 0, 0)
    weight_sums(1, 1)
    stage(0, 0, 1, 3)
    pair_sum(1, 0)
    stage(1, 0, 1, 0)
    stage(1, 0, 0, 0)
    weight_sums(2, 0)
    pair_sum(1, 1)
    stage(1, 1, 1, 0)
    stage(1, 1, 0, 0)
    stage(0, 0, 0, 3)
    weight_sums(2, 1)
    stage(0, 1, 1, 1)
    stage(0, 1, 0, 1)
    stage(0, 0, 1, 4)
    pair_sum(2, 0)
    stage(2, 0, 1, 0)
    stage(2, 0, 0, 0)
    stage(1, 0, 1, 1)
    input_part(opp)
    stage(1, 0, 0, 1)
    pair_sum(2, 1)
    stage(2, 1, 1, 0)
    stage(2, 1, 0, 0)
    stage(1, 1, 1, 1)
    x_start()
    input_part(prv)
    stage(0, 0, 0, 4)
    input_part(nxt)
    stage(1, 1, 0, 1)
    stage(2, 0, 1, 1)
    stage(0, 1, 1, 2)
    stage(1, 0, 1, 2)
    stage(0, 1, 0, 2)
    stage(2, 1, 1, 1)
    stage(0, 0, 1, 5)
    stage(1, 1, 1, 2)
    stage(2, 0, 1, 2)
    stage(0, 1, 1, 3)
    stage(2, 0, 0, 1)
    stage(1, 0, 1, 3)
    x_forward()
    stage(1, 0, 0, 2)
    stage(0, 1, 0, 3)
    stage(2, 1, 1, 2)
    stage(2, 1, 0, 1)
    stage(1, 1, 1, 3)
    stage(1, 1, 0, 2)
    stage(2, 0, 1, 3)
    stage(2, 0, 0, 2)
    stage(0, 1, 1, 4)
    stage(1, 0, 1, 4)
    stage(2, 1, 0, 2)
    stage(1, 0, 0, 3)
    stage(2, 1, 1, 3)
    stage(0, 1, 0, 4)
    stage(0, 1, 1, 5)
    stage(1, 1, 1, 4)
    stage(1, 0, 1, 5)
    stage(1, 1, 0, 3)
    stage(2, 0, 1, 4)
    stage(2, 0, 0, 3)
    stage(1, 1, 1, 5)
    stage(2, 1, 0, 3)
    stage(2, 1, 1, 4)
    stage(1, 0, 0, 4)
    stage(2, 0, 1, 5)
    stage(1, 1, 0, 4)
    x_finish()
    stage(2, 0, 0, 4)
    stage(2, 1, 1, 5)
    stage(2, 1, 0, 4)

    for a in range(3):
        for way in range(2):
            for k in range(2):
                gather(a, way, k, x, k if way == 0 else 1 - k).wait_send()
            gather(a, way, 2, came[way], way).wait_send()
    for way in range(2):
        x_first(way).wait_send()
        x_second(way).wait_send()
    for k in range(3):
        for i in range(nz // zt):
            pair(k, i).wait_send()
        for e in range(2):
            for way, step in ((0, 0), (0, 1), (1, 0)):
                a_y(k, e, way, step).wait_send()

    def sent(k, e, names, steps, direct):
        for name in names:
            a_z(k, e, name).wait_send()
        for way, step in steps:
            b_z(k, e, way, step).wait_send()
        for m in direct:
            b_y(k, e, m).wait_send()

    for e in range(2):

        def yes():
            for k in range(3):
                sent(k, e, "afd", ((0, 0), (0, 2), (1, 1)), range(3))

        def no():
            for k in range(3):
                sent(k, e, "bceg", ((0, 1), (0, 3), (1, 0), (1, 2)), ())

        on_parity(e, yes, no)


def written(*refs):
    n = (len(refs) - 1) // 2
    copies = [pltpu.make_async_copy(refs[k], refs[n + k], refs[-1].at[k]) for k in range(n)]
    for copy in copies:
        copy.start()
    for copy in copies:
        copy.wait()


def solution(mesh):
    n_rep = mesh.shape["rep"]
    nz = n_rep // NY
    nx = mesh.shape["fs"]
    cores = mesh.shape["tp"]

    def on_device(tokens, cotangent, gate_weight, up_weight, down_weight_t):
        rows, d = tokens.shape
        ff = gate_weight.shape[1]
        scale = float(rows * n_rep * nx * cores) ** (-0.5)
        lines = d // (n_rep * cores)
        wb = tuple(ff - w for w in WIDTH_A)
        shapes = (((rows, d), BF16),) + (((lines, ff), F32),) * 3
        vmem = pl.BlockSpec(memory_space=pltpu.VMEM)
        dma = pltpu.SemaphoreType.DMA
        results = pl.pallas_call(
            functools.partial(body, nz, scale),
            out_shape=tuple(pltpu.VMEM(*s) for s in shapes),
            in_specs=[pl.BlockSpec(memory_space=pl.ANY)] * 5,
            out_specs=(vmem,) * 4,
            scratch_shapes=[
                pltpu.VMEM((nx, rows, d), BF16),
                pltpu.VMEM((2, nx, rows, d // 2), BF16),
                pltpu.VMEM((d, nx * rows), BF16),
                pltpu.VMEM((d, nx * rows), BF16),
                pltpu.VMEM((d, ff), BF16),
                pltpu.VMEM((d, ff), BF16),
                pltpu.VMEM((d, ff), BF16),
                pltpu.VMEM((ff, d), BF16),
                pltpu.VMEM((ff, d), BF16),
                pltpu.VMEM((nx, rows, ff), F32),
                pltpu.VMEM((nx, rows, ff), F32),
                pltpu.VMEM((nx, rows, ff), F32),
                pltpu.VMEM((nx * rows, ff), BF16),
                pltpu.VMEM((nx * rows, ff), BF16),
                pltpu.VMEM((nx * rows, ff), BF16),
                pltpu.VMEM((nx, rows, d), BF16),
                pltpu.VMEM((2, rows // 2, d), BF16),
                pltpu.VMEM((2, rows, d), BF16),
                pltpu.VMEM((3, nz, NY, cores, lines, ff), BF16),
                pltpu.VMEM((3, nz, NY, lines, ff), BF16),
                *[pltpu.VMEM((nz, NY, lines, w), BF16) for w in WIDTH_A],
                *[pltpu.VMEM((nz, NY, lines, w), BF16) for w in wb],
                *[pltpu.VMEM((3, nz, lines, w), BF16) for w in WIDTH_A],
                *[pltpu.VMEM((7, lines, w), BF16) for w in WIDTH_A],
                *[pltpu.VMEM((7, NY, lines, w), BF16) for w in wb],
                *[pltpu.VMEM((3, lines, w), BF16) for w in wb],
                dma((3 + 2 * nz,)),
                dma((3, 2, 3)),
                dma((3, 2, 3)),
                dma((3, nz // 2)),
                dma((3, nz // 2)),
                dma((4,)),
                dma((4,)),
                dma((12, 10)),
                dma((12, 10)),
            ],
            compiler_params=pltpu.CompilerParams(
                collective_id=0, has_side_effects=True, vmem_limit_bytes=60 * 1024 * 1024
            ),
        )(tokens, cotangent, gate_weight, up_weight, down_weight_t)
        return pl.pallas_call(
            written,
            out_shape=tuple(jax.ShapeDtypeStruct(*s) for s in shapes),
            in_specs=[vmem] * 4,
            out_specs=(pl.BlockSpec(memory_space=pltpu.HBM),) * 4,
            scratch_shapes=[dma((4,))],
        )(*[pltpu.with_memory_space_constraint(r, pltpu.VMEM) for r in results])

    return jax.shard_map(
        on_device,
        mesh=mesh,
        in_specs=(
            P(("rep", "fs", "tp"), None),
            P(("rep", "fs", "tp"), None),
            P(None, "fs"),
            P(None, "fs"),
            P(None, "fs"),
        ),
        out_specs=(
            P(("rep", "fs", "tp"), None),
            P(("rep", "tp"), "fs"),
            P(("rep", "tp"), "fs"),
            P(("rep", "tp"), "fs"),
        ),
        check_vma=False,
    )
```

```python
import functools

import jax
import jax.numpy as jnp
from jax import lax
from jax.experimental import pallas as pl
from jax.experimental.pallas import tpu as pltpu
from jax.sharding import PartitionSpec as P

MESH = pl.DeviceIdType.MESH
F32 = jnp.float32
BF16 = jnp.bfloat16
NY = 4
WIDTH_A = (384, 384, 640)


def body(
    nz, scale, tok_hbm, cot_hbm, gw_hbm, uw_hbm, dw_hbm, ig_ref, gg_ref, ug_ref, dg_ref,
    tok, cot, tokt, cott, gw, uw, dw, gwt, uwt, gpre, upre, hpre, hid, gb, ub, part, xhalf, xfull,
    prod, peer, *rest,
):
    sa, sb, ya, za, zb, yb = (rest[3 * i : 3 * i + 3] for i in range(6))
    ld_sem, ag_s, ag_r, dd_s, dd_r, xs_s, xs_r, rs_s, rs_r = rest[18:]
    rep = lax.axis_index("rep")
    x = lax.axis_index("fs")
    t = lax.axis_index("tp")
    nx = 4
    rows = tok.shape[1]
    half = rows // 2
    d, ff = gw.shape
    hd = d // 2
    zw = d // nz
    hz = nz // 2
    z = rep // NY
    y = lax.rem(rep, NY)
    nxt, prv, opp = lax.rem(x + 1, nx), lax.rem(x + nx - 1, nx), lax.rem(x + 2, nx)
    other = 1 - t
    sgn = 1 - 2 * t

    def along_y(step):
        return lax.rem(y + NY + step, NY)

    def along_z(step):
        return lax.rem(z + nz + step, nz)

    def place(zi):
        return zi % 2 * hz + zi // 2 if isinstance(zi, int) else lax.rem(zi, 2) * hz + zi // 2

    def dev_y(step):
        return {"rep": z * NY + along_y(step)}

    def dev_z(step):
        return {"rep": along_z(step) * NY + y}

    def on_parity(e, yes, no=None):
        mine = lax.rem(z, 2) == e
        pl.when(mine)(yes)
        if no is not None:
            pl.when(jnp.logical_not(mine))(no)

    parts = [(tok_hbm, tok.at[x]), (gw_hbm, gw), (uw_hbm, uw)]
    for zi in range(nz):
        cols = pl.ds(zi * zw, zw)
        parts.append((cot_hbm.at[:, cols], cot.at[zi % 2, x, :, pl.ds(zi // 2 * zw, zw)]))
    for zi in range(nz):
        parts.append((dw_hbm.at[pl.ds(zi * zw, zw), :], dw.at[pl.ds(place(zi) * zw, zw), :]))
    loads = [pltpu.make_async_copy(src, dst, ld_sem.at[k]) for k, (src, dst) in enumerate(parts)]
    for load in loads:
        load.start()

    barrier = pltpu.get_barrier_semaphore()
    peers = [{"fs": nxt}, {"fs": prv}, {"tp": other}]
    peers += [dev_y(s) for s in (1, -1, 2)] + [dev_z(s) for s in (1, -1, 2, -2)]
    for who in peers:
        pl.semaphore_signal(barrier, inc=1, device_id=who, device_id_type=MESH)
    pl.semaphore_wait(barrier, len(peers))

    def remote(src, dst, s, r, who):
        return pltpu.make_async_remote_copy(
            src_ref=src, dst_ref=dst, send_sem=s, recv_sem=r, device_id=who, device_id_type=MESH
        )

    bufs = (tok, cot.at[0], cot.at[1])
    to = ({"fs": nxt}, {"fs": prv})
    came = (prv, nxt)

    def gather(a, way, k, slot, h):
        ref = bufs[a].at[slot, pl.ds(h * half, half), :]
        return remote(ref, ref, ag_s.at[a, way, k], ag_r.at[a, way, k], to[way])

    def gather_out(a):
        for k in range(2):
            for way in range(2):
                gather(a, way, k, x, k if way == 0 else 1 - k).start()

    def gather_in(a, way, k):
        if k == 2:
            gather(a, way, 2, opp, way).wait_recv()
        else:
            gather(a, way, k, came[way], k if way == 0 else 1 - k).wait_recv()

    def pass_on(a):
        for way in range(2):
            gather_in(a, way, 0)
            gather(a, way, 2, came[way], way).start()

    nt = 256

    def rows_of(slot):
        return pl.ds(pl.multiple_of(slot * rows, rows), rows)

    def turned_cot(e, slot):
        cott[e * hd : (e + 1) * hd, rows_of(slot)] = cot[e, slot].T

    def turn_weights():
        def one(i, _):
            lines = pl.ds(pl.multiple_of(i * nt, nt), nt)
            gwt[:, lines] = gw[lines, :].T
            uwt[:, lines] = uw[lines, :].T
            return 0

        lax.fori_loop(0, d // nt, one, 0)

    def forward(slot):
        at = rows_of(slot)
        for i in range(ff // nt):
            cols = pl.ds(i * nt, nt)
            g = jnp.dot(tok[slot], gw[:, cols], preferred_element_type=F32)
            u = jnp.dot(tok[slot], uw[:, cols], preferred_element_type=F32)
            gpre[slot, :, cols] = g
            upre[slot, :, cols] = u
            hid[at, cols] = (g * jax.nn.sigmoid(g) * u).astype(BF16)
        for zi in range(nz):
            tokt[place(zi) * zw : (place(zi) + 1) * zw, at] = tok[slot, :, zi * zw : (zi + 1) * zw].T

    def hid_part(slot):
        for i in range(ff // nt):
            cols = pl.ds(i * nt, nt)
            hpre[slot, :, cols] = jnp.dot(cot[0, slot], dw[0:hd, cols], preferred_element_type=F32)

    def backward(slot):
        at = rows_of(slot)
        for i in range(ff // nt):
            cols = pl.ds(i * nt, nt)
            h = hpre[slot, :, cols] + jnp.dot(cot[1, slot], dw[hd:d, cols], preferred_element_type=F32)
            g = gpre[slot, :, cols]
            sig = jax.nn.sigmoid(g)
            gb[at, cols] = (h * upre[slot, :, cols] * sig * (1.0 + g * (1.0 - sig))).astype(BF16)
            ub[at, cols] = (h * (g * sig)).astype(BF16)

    def input_part(slot):
        at = rows_of(slot)
        for i in range(d // nt):
            cols = pl.ds(i * nt, nt)
            p = jnp.dot(gb[at, :], gwt[:, cols], preferred_element_type=F32)
            p += jnp.dot(ub[at, :], uwt[:, cols], preferred_element_type=F32)
            part[slot, :, cols] = p.astype(BF16)

    def x_first(way):
        return remote(
            part.at[opp, pl.ds(way * half, half), :], xhalf.at[way], xs_s.at[way], xs_r.at[way], to[way]
        )

    def x_second(way):
        return remote(part.at[(nxt, prv)[way]], xfull.at[way], xs_s.at[2 + way], xs_r.at[2 + way], to[way])

    def x_start():
        for way in range(2):
            x_first(way).start()

    def x_forward():
        for way in range(2):
            x_first(way).wait_recv()
            slot = (nxt, prv)[way]
            for i in range(half // 16):
                at = pl.ds(way * half + i * 16, 16)
                got = xhalf[way, pl.ds(i * 16, 16), :].astype(F32)
                part[slot, at, :] = (part[slot, at, :].astype(F32) + got).astype(BF16)
            x_second(way).start()

    def x_finish():
        for way in range(2):
            x_second(way).wait_recv()

        def one(i, _):
            at = pl.ds(pl.multiple_of(i * 16, 16), 16)
            total = part[x, at, :].astype(F32) + xfull[0, at, :].astype(F32) + xfull[1, at, :].astype(F32)
            ig_ref[at, :] = total.astype(BF16)
            return 0

        lax.fori_loop(0, rows // 16, one, 0)

    zt = 2

    def pair(k, i):
        at = pl.ds(i * zt, zt)
        return remote(prod.at[k, at, :, other], peer.at[k, at], dd_s.at[k, i], dd_r.at[k, i], {"tp": other})

    left, right, outs = (cott, tokt, tokt), (hid, gb, ub), (dg_ref, gg_ref, ug_ref)

    def weight_sums(k, e):
        for i in range(e * hz // zt, (e + 1) * hz // zt):
            lines = pl.ds(i * zt * zw, zt * zw)
            for j in range(ff // nt):
                cols = pl.ds(j * nt, nt)
                acc = jnp.dot(left[k][lines, :], right[k][:, cols], preferred_element_type=F32)
                prod[k, i * zt : (i + 1) * zt, :, :, :, cols] = acc.astype(BF16).reshape(zt, NY, 2, 32, nt)
            pair(k, i).start()

    def pair_sum(k, e):
        for i in range(e * hz // zt, (e + 1) * hz // zt):
            pair(k, i).wait_recv()
        wa = WIDTH_A[k]

        def one(i, _):
            for j in range(NY):
                both = prod[k, i, j, t].astype(F32) + peer[k, i, j].astype(F32)
                both = both.astype(BF16)
                sa[k][i, j] = both[:, :wa]
                sb[k][i, j] = both[:, wa:]
            return 0

        lax.fori_loop(e * hz, (e + 1) * hz, one, 0)

    ly, lz = (2, 1), (4, 3)

    def sems(k, e, h, n):
        u = (k * 2 + e) * 2 + h
        return rs_s.at[u, n], rs_r.at[u, n]

    def go(way):
        return sgn if way == 0 else -sgn

    def a_y(k, e, way, step):
        m = step if way == 0 else 2
        at = pl.ds(e * hz, hz)
        dest = along_y((ly[way] - step) * go(way))
        return remote(sa[k].at[at, dest], ya[k].at[m, at], *sems(k, e, 0, m), dev_y(go(way)))

    hops = {"a": (4, 2), "b": (3, 1), "c": (1, 1), "d": (2, 2), "e": (-3, -2), "f": (-2, -1), "g": (-1, -1)}

    def a_z(k, e, name):
        m = "abcdefg".index(name)
        owner, target = hops[name]
        src = sa[k].at[place(along_z(owner * sgn)), y]
        return remote(src, za[k].at[m], *sems(k, e, 0, 3 + m), dev_z(target * sgn))

    def b_z(k, e, way, step):
        m = step if way == 0 else lz[0] + step
        src = sb[k].at[place(along_z((lz[way] - step) * go(way)))]
        return remote(src, zb[k].at[m], *sems(k, e, 1, m), dev_z(go(way)))

    y_steps = (1, -1, 2)

    def b_y(k, e, m):
        src = sb[k].at[place(z), along_y(y_steps[m])]
        return remote(src, yb[k].at[m], *sems(k, e, 1, 7 + m), dev_y(y_steps[m]))

    def added(ref, at, arrived):
        v = ref[at].astype(F32)
        for got in arrived:
            v += got.astype(F32)
        return v

    def a_stage(k, e, n):
        names = "abcdefg"
        if n <= 1:
            for way in range(2):
                if n >= ly[way]:
                    continue
                if n == 1:
                    a_y(k, e, way, 0).wait_recv()
                    at = along_y((ly[way] - 1) * go(way))
                    for i in range(e * hz, (e + 1) * hz):
                        sa[k][i, at] = added(sa[k], (i, at), [ya[k][0, i]]).astype(BF16)
                a_y(k, e, way, n).start()
        elif n == 2:
            a_y(k, e, 0, 1).wait_recv()
            a_y(k, e, 1, 0).wait_recv()
            for i in range(e * hz, (e + 1) * hz):
                sa[k][i, y] = added(sa[k], (i, y), [ya[k][1, i], ya[k][2, i]]).astype(BF16)

            def yes():
                for name in "af":
                    a_z(k, e, name).start()

            def no():
                for name in "ecb":
                    a_z(k, e, name).start()

            on_parity(e, yes, no)
        elif n == 3:

            def relay(one, two, step, out):
                a_z(k, e, one).wait_recv()
                a_z(k, e, two).wait_recv()
                at = (place(along_z(step * sgn)), y)
                got = [za[k][names.index(one)], za[k][names.index(two)]]
                sa[k][at] = added(sa[k], at, got).astype(BF16)
                a_z(k, e, out).start()

            on_parity(e, lambda: relay("a", "b", 2, "d"), lambda: relay("e", "f", -1, "g"))
        else:

            def end():
                for name in "cdg":
                    a_z(k, e, name).wait_recv()
                v = added(sa[k], (place(z), y), [za[k][names.index(c)] for c in "cdg"])
                outs[k][:, : WIDTH_A[k]] = v * scale

            on_parity(e, end)

    def b_sum(k, at, ms):
        for j in range(NY):
            sb[k][at, j] = added(sb[k], (at, j), [zb[k][m, j] for m in ms]).astype(BF16)

    def b_stage(k, e, n):
        if n <= 3:

            def step(way):
                if n > 0:
                    b_z(k, e, way, n - 1).wait_recv()
                    m = n - 1 if way == 0 else lz[0] + n - 1
                    b_sum(k, place(along_z((lz[way] - n) * go(way))), [m])
                b_z(k, e, way, n).start()

            def steps(rest_of):
                def run():
                    for way in range(2):
                        if n < lz[way] and (lz[way] - n) % 2 == rest_of:
                            step(way)

                return run

            on_parity(e, steps(0), steps(1))
        elif n == 4:

            def turn():
                b_z(k, e, 0, 3).wait_recv()
                b_z(k, e, 1, 2).wait_recv()
                b_sum(k, place(z), [3, 6])
                for m in range(3):
                    b_y(k, e, m).start()

            on_parity(e, turn)
        else:

            def end():
                for m in range(3):
                    b_y(k, e, m).wait_recv()
                v = added(sb[k], (place(z), y), [yb[k][m] for m in range(3)])
                outs[k][:, WIDTH_A[k] :] = v * scale

            on_parity(e, end)

    def stage(k, e, h, n):
        (a_stage, b_stage)[h](k, e, n)

    loads[0].wait()
    gather_out(0)
    loads[1].wait()
    loads[2].wait()
    forward(x)
    turn_weights()
    pass_on(0)
    for load in loads[3 : 3 + nz]:
        load.wait()
    gather_out(1)
    for load in loads[3 + nz :]:
        load.wait()
    hid_part(x)
    turned_cot(0, x)
    backward(x)
    turned_cot(1, x)
    input_part(x)
    gather_in(0, 0, 1)
    forward(prv)
    gather_in(0, 1, 1)
    forward(nxt)
    gather_in(0, 0, 2)
    gather_in(0, 1, 2)
    forward(opp)
    pass_on(1)
    gather_out(2)
    gather_in(1, 0, 1)
    hid_part(prv)
    turned_cot(0, prv)
    gather_in(1, 1, 1)
    hid_part(nxt)
    turned_cot(0, nxt)
    gather_in(1, 0, 2)
    gather_in(1, 1, 2)
    turned_cot(0, opp)
    weight_sums(0, 0)
    pass_on(2)
    pair_sum(0, 0)
    stage(0, 0, 0, 0)
    stage(0, 0, 1, 0)
    gather_in(2, 0, 1)
    gather_in(2, 1, 1)
    backward(nxt)
    turned_cot(1, nxt)
    backward(prv)
    turned_cot(1, prv)
    hid_part(opp)
    stage(0, 0, 1, 1)
    gather_in(2, 0, 2)
    gather_in(2, 1, 2)
    turned_cot(1, opp)
    weight_sums(0, 1)
    backward(opp)
    stage(0, 0, 0, 1)
    weight_sums(1, 0)
    pair_sum(0, 1)
    stage(0, 1, 0, 0)
    stage(0, 1, 1, 0)
    weight_sums(1, 1)
    pair_sum(1, 0)
    stage(1, 0, 1, 0)
    stage(1, 0, 0, 0)
    stage(0, 0, 1, 2)
    weight_sums(2, 0)
    pair_sum(1, 1)
    stage(1, 1, 0, 0)
    stage(1, 1, 1, 0)
    weight_sums(2, 1)
    stage(0, 0, 0, 2)
    stage(0, 1, 1, 1)
    pair_sum(2, 0)
    input_part(opp)
    stage(2, 0, 1, 0)
    stage(2, 0, 0, 0)
    stage(1, 1, 1, 1)
    pair_sum(2, 1)
    stage(1, 0, 1, 1)
    stage(0, 0, 1, 3)
    x_start()
    stage(1, 1, 0, 1)
    stage(2, 1, 1, 0)
    stage(2, 0, 1, 1)
    stage(0, 1, 0, 1)
    stage(0, 1, 1, 2)
    input_part(prv)
    stage(2, 1, 0, 0)
    stage(1, 0, 0, 1)
    input_part(nxt)
    stage(1, 0, 1, 2)
    stage(0, 0, 0, 3)
    stage(1, 1, 1, 2)
    stage(2, 1, 1, 1)
    stage(2, 0, 1, 2)
    stage(2, 0, 0, 1)
    stage(1, 1, 0, 2)
    stage(0, 1, 1, 3)
    stage(1, 0, 1, 3)
    stage(0, 1, 0, 2)
    x_forward()
    stage(2, 1, 1, 2)
    stage(2, 1, 0, 1)
    stage(1, 1, 1, 3)
    stage(2, 0, 1, 3)
    stage(1, 0, 0, 2)
    stage(2, 0, 0, 2)
    stage(1, 0, 1, 4)
    stage(2, 1, 1, 3)
    stage(2, 1, 0, 2)
    stage(0, 1, 0, 3)
    stage(2, 1, 1, 4)
    stage(0, 1, 1, 4)
    stage(1, 0, 1, 5)
    stage(2, 0, 0, 3)
    stage(1, 1, 1, 4)
    stage(1, 1, 0, 3)
    stage(0, 0, 1, 4)
    stage(1, 0, 0, 3)
    stage(2, 0, 1, 4)
    stage(2, 1, 0, 3)
    stage(2, 1, 1, 5)
    x_finish()
    stage(0, 0, 0, 4)
    stage(2, 0, 0, 4)
    stage(2, 0, 1, 5)
    stage(0, 0, 1, 5)
    stage(1, 1, 1, 5)
    stage(1, 1, 0, 4)
    stage(1, 0, 0, 4)
    stage(0, 1, 1, 5)
    stage(0, 1, 0, 4)
    stage(2, 1, 0, 4)

    for a in range(3):
        for way in range(2):
            for k in range(2):
                gather(a, way, k, x, k if way == 0 else 1 - k).wait_send()
            gather(a, way, 2, came[way], way).wait_send()
    for way in range(2):
        x_first(way).wait_send()
        x_second(way).wait_send()
    for k in range(3):
        for i in range(nz // zt):
            pair(k, i).wait_send()
        for e in range(2):
            for way, step in ((0, 0), (0, 1), (1, 0)):
                a_y(k, e, way, step).wait_send()

    def sent(k, e, names, steps, direct):
        for name in names:
            a_z(k, e, name).wait_send()
        for way, step in steps:
            b_z(k, e, way, step).wait_send()
        for m in direct:
            b_y(k, e, m).wait_send()

    for e in range(2):

        def yes():
            for k in range(3):
                sent(k, e, "afd", ((0, 0), (0, 2), (1, 1)), range(3))

        def no():
            for k in range(3):
                sent(k, e, "bceg", ((0, 1), (0, 3), (1, 0), (1, 2)), ())

        on_parity(e, yes, no)


def written(*refs):
    n = (len(refs) - 1) // 2
    copies = [pltpu.make_async_copy(refs[k], refs[n + k], refs[-1].at[k]) for k in range(n)]
    for copy in copies:
        copy.start()
    for copy in copies:
        copy.wait()


def solution(mesh):
    n_rep = mesh.shape["rep"]
    nz = n_rep // NY
    nx = mesh.shape["fs"]
    cores = mesh.shape["tp"]

    def on_device(tokens, cotangent, gate_weight, up_weight, down_weight_t):
        rows, d = tokens.shape
        ff = gate_weight.shape[1]
        scale = float(rows * n_rep * nx * cores) ** (-0.5)
        lines = d // (n_rep * cores)
        wb = tuple(ff - w for w in WIDTH_A)
        shapes = (((rows, d), BF16),) + (((lines, ff), F32),) * 3
        vmem = pl.BlockSpec(memory_space=pltpu.VMEM)
        dma = pltpu.SemaphoreType.DMA
        results = pl.pallas_call(
            functools.partial(body, nz, scale),
            out_shape=tuple(pltpu.VMEM(*s) for s in shapes),
            in_specs=[pl.BlockSpec(memory_space=pl.ANY)] * 5,
            out_specs=(vmem,) * 4,
            scratch_shapes=[
                pltpu.VMEM((nx, rows, d), BF16),
                pltpu.VMEM((2, nx, rows, d // 2), BF16),
                pltpu.VMEM((d, nx * rows), BF16),
                pltpu.VMEM((d, nx * rows), BF16),
                pltpu.VMEM((d, ff), BF16),
                pltpu.VMEM((d, ff), BF16),
                pltpu.VMEM((d, ff), BF16),
                pltpu.VMEM((ff, d), BF16),
                pltpu.VMEM((ff, d), BF16),
                pltpu.VMEM((nx, rows, ff), F32),
                pltpu.VMEM((nx, rows, ff), F32),
                pltpu.VMEM((nx, rows, ff), F32),
                pltpu.VMEM((nx * rows, ff), BF16),
                pltpu.VMEM((nx * rows, ff), BF16),
                pltpu.VMEM((nx * rows, ff), BF16),
                pltpu.VMEM((nx, rows, d), BF16),
                pltpu.VMEM((2, rows // 2, d), BF16),
                pltpu.VMEM((2, rows, d), BF16),
                pltpu.VMEM((3, nz, NY, cores, lines, ff), BF16),
                pltpu.VMEM((3, nz, NY, lines, ff), BF16),
                *[pltpu.VMEM((nz, NY, lines, w), BF16) for w in WIDTH_A],
                *[pltpu.VMEM((nz, NY, lines, w), BF16) for w in wb],
                *[pltpu.VMEM((3, nz, lines, w), BF16) for w in WIDTH_A],
                *[pltpu.VMEM((7, lines, w), BF16) for w in WIDTH_A],
                *[pltpu.VMEM((7, NY, lines, w), BF16) for w in wb],
                *[pltpu.VMEM((3, lines, w), BF16) for w in wb],
                dma((3 + 2 * nz,)),
                dma((3, 2, 3)),
                dma((3, 2, 3)),
                dma((3, nz // 2)),
                dma((3, nz // 2)),
                dma((4,)),
                dma((4,)),
                dma((12, 10)),
                dma((12, 10)),
            ],
            compiler_params=pltpu.CompilerParams(
                collective_id=0, has_side_effects=True, vmem_limit_bytes=60 * 1024 * 1024
            ),
        )(tokens, cotangent, gate_weight, up_weight, down_weight_t)
        return pl.pallas_call(
            written,
            out_shape=tuple(jax.ShapeDtypeStruct(*s) for s in shapes),
            in_specs=[vmem] * 4,
            out_specs=(pl.BlockSpec(memory_space=pltpu.HBM),) * 4,
            scratch_shapes=[dma((4,))],
        )(*[pltpu.with_memory_space_constraint(r, pltpu.VMEM) for r in results])

    return jax.shard_map(
        on_device,
        mesh=mesh,
        in_specs=(
            P(("rep", "fs", "tp"), None),
            P(("rep", "fs", "tp"), None),
            P(None, "fs"),
            P(None, "fs"),
            P(None, "fs"),
        ),
        out_specs=(
            P(("rep", "fs", "tp"), None),
            P(("rep", "tp"), "fs"),
            P(("rep", "tp"), "fs"),
            P(("rep", "tp"), "fs"),
        ),
        check_vma=False,
    )
```

```python
import functools

import jax
import jax.numpy as jnp
from jax import lax
from jax.experimental import pallas as pl
from jax.experimental.pallas import tpu as pltpu
from jax.sharding import PartitionSpec as P

MESH = pl.DeviceIdType.MESH
F32 = jnp.float32
BF16 = jnp.bfloat16
NY = 4
WIDTH_A = (384, 384, 512)
CHAINED = (0, 1)
OWN, NXT, PRV, OPP = range(4)


def body(
    nz, scale, tok_hbm, cot_hbm, gw_hbm, uw_hbm, dw_hbm, ig_ref, gg_ref, ug_ref, dg_ref,
    tok, cot, tokt, cott, gw, uw, dw, gwt, uwt, gpre, upre, hpre, hid, gb, ub, part, xhalf, xfull,
    prod, peer, *rest,
):
    sa, sb, ya, za, zb, yb = (rest[3 * i : 3 * i + 3] for i in range(6))
    ld_sem, ag_s, ag_r, dd_s, dd_r, xs_s, xs_r, rs_s, rs_r = rest[18:]
    rep = lax.axis_index("rep")
    x = lax.axis_index("fs")
    t = lax.axis_index("tp")
    nx = 4
    rows = tok.shape[1]
    half = rows // 2
    d, ff = gw.shape
    hd = d // 2
    zw = d // nz
    hz = nz // 2
    z = rep // NY
    y = lax.rem(rep, NY)
    nxt, prv = lax.rem(x + 1, nx), lax.rem(x + nx - 1, nx)
    other = 1 - t
    sgn = 1 - 2 * t

    def along_y(step):
        return lax.rem(y + NY + step, NY)

    def along_z(step):
        return lax.rem(z + nz + step, nz)

    def place(zi):
        return zi % 2 * hz + zi // 2 if isinstance(zi, int) else lax.rem(zi, 2) * hz + zi // 2

    def dev_y(step):
        return {"rep": z * NY + along_y(step)}

    def dev_z(step):
        return {"rep": along_z(step) * NY + y}

    def on_parity(e, yes, no=None):
        mine = lax.rem(z, 2) == e
        pl.when(mine)(yes)
        if no is not None:
            pl.when(jnp.logical_not(mine))(no)

    parts = [(tok_hbm, tok.at[OWN]), (gw_hbm, gw), (uw_hbm, uw)]
    for zi in range(nz):
        cols = pl.ds(zi * zw, zw)
        parts.append((cot_hbm.at[:, cols], cot.at[zi % 2, OWN, :, pl.ds(zi // 2 * zw, zw)]))
    for zi in range(nz):
        parts.append((dw_hbm.at[pl.ds(zi * zw, zw), :], dw.at[pl.ds(place(zi) * zw, zw), :]))
    loads = [pltpu.make_async_copy(src, dst, ld_sem.at[k]) for k, (src, dst) in enumerate(parts)]
    for load in loads:
        load.start()

    barrier = pltpu.get_barrier_semaphore()
    peers = [{"fs": nxt}, {"fs": prv}, {"tp": other}]
    peers += [dev_y(s) for s in (1, -1, 2)] + [dev_z(s) for s in (1, -1, 2, -2)]
    for who in peers:
        pl.semaphore_signal(barrier, inc=1, device_id=who, device_id_type=MESH)
    pl.semaphore_wait(barrier, len(peers))

    def remote(src, dst, s, r, who):
        return pltpu.make_async_remote_copy(
            src_ref=src, dst_ref=dst, send_sem=s, recv_sem=r, device_id=who, device_id_type=MESH
        )

    bufs = (tok, cot.at[0], cot.at[1])
    to = ({"fs": nxt}, {"fs": prv})
    came = (PRV, NXT)

    def gather(a, way, k):
        h = way if k == 2 else (k if way == 0 else 1 - k)
        at = pl.ds(h * half, half)
        src, dst = (came[way], OPP) if k == 2 else (OWN, came[way])
        return remote(
            bufs[a].at[src, at, :], bufs[a].at[dst, at, :], ag_s.at[a, way, k], ag_r.at[a, way, k], to[way]
        )

    def gather_out(a):
        for k in range(2):
            for way in range(2):
                gather(a, way, k).start()

    def gather_in(a, way, k):
        gather(a, way, k).wait_recv()

    def pass_on(a):
        for way in range(2):
            gather_in(a, way, 0)
            gather(a, way, 2).start()

    nt = 256

    def rows_of(slot):
        return pl.ds(slot * rows, rows)

    def turned_cot(e, slot):
        cott[e * hd : (e + 1) * hd, rows_of(slot)] = cot[e, slot].T

    def turn_weights():
        def one(i, _):
            lines = pl.ds(pl.multiple_of(i * nt, nt), nt)
            gwt[:, lines] = gw[lines, :].T
            uwt[:, lines] = uw[lines, :].T
            return 0

        lax.fori_loop(0, d // nt, one, 0)

    def forward(slot):
        at = rows_of(slot)
        for i in range(ff // nt):
            cols = pl.ds(i * nt, nt)
            g = jnp.dot(tok[slot], gw[:, cols], preferred_element_type=F32)
            u = jnp.dot(tok[slot], uw[:, cols], preferred_element_type=F32)
            gpre[slot, :, cols] = g
            upre[slot, :, cols] = u
            hid[at, cols] = (g * jax.nn.sigmoid(g) * u).astype(BF16)
        for zi in range(nz):
            tokt[place(zi) * zw : (place(zi) + 1) * zw, at] = tok[slot, :, zi * zw : (zi + 1) * zw].T

    def hid_part(slot):
        for i in range(ff // nt):
            cols = pl.ds(i * nt, nt)
            hpre[slot, :, cols] = jnp.dot(cot[0, slot], dw[0:hd, cols], preferred_element_type=F32)

    def backward(slot):
        at = rows_of(slot)
        for i in range(ff // nt):
            cols = pl.ds(i * nt, nt)
            h = hpre[slot, :, cols] + jnp.dot(cot[1, slot], dw[hd:d, cols], preferred_element_type=F32)
            g = gpre[slot, :, cols]
            sig = jax.nn.sigmoid(g)
            gb[at, cols] = (h * upre[slot, :, cols] * sig * (1.0 + g * (1.0 - sig))).astype(BF16)
            ub[at, cols] = (h * (g * sig)).astype(BF16)

    def input_part(slot):
        at = rows_of(slot)
        for i in range(d // nt):
            cols = pl.ds(i * nt, nt)
            p = jnp.dot(gb[at, :], gwt[:, cols], preferred_element_type=F32)
            p += jnp.dot(ub[at, :], uwt[:, cols], preferred_element_type=F32)
            part[slot, :, cols] = p.astype(BF16)

    def x_first(way):
        return remote(
            part.at[OPP, pl.ds(way * half, half), :], xhalf.at[way], xs_s.at[way], xs_r.at[way], to[way]
        )

    def x_second(way, direct):
        at = pl.ds((1 - way if direct else way) * half, half)
        n = (4 if direct else 2) + way
        return remote(part.at[(NXT, PRV)[way], at, :], xfull.at[way, at, :], xs_s.at[n], xs_r.at[n], to[way])

    def x_direct():
        for way in range(2):
            x_second(way, True).start()

    def x_start():
        for way in range(2):
            x_first(way).start()

    def x_forward():
        for way in range(2):
            x_first(way).wait_recv()
            slot = (NXT, PRV)[way]
            for i in range(half // 16):
                at = pl.ds(way * half + i * 16, 16)
                got = xhalf[way, pl.ds(i * 16, 16), :].astype(F32)
                part[slot, at, :] = (part[slot, at, :].astype(F32) + got).astype(BF16)
            x_second(way, False).start()

    def x_finish():
        for way in range(2):
            x_second(way, True).wait_recv()
            x_second(way, False).wait_recv()

        def one(i, _):
            at = pl.ds(pl.multiple_of(i * 16, 16), 16)
            total = part[OWN, at, :].astype(F32) + xfull[0, at, :].astype(F32) + xfull[1, at, :].astype(F32)
            ig_ref[at, :] = total.astype(BF16)
            return 0

        lax.fori_loop(0, rows // 16, one, 0)

    zt = 2

    def pair(k, i):
        at = pl.ds(i * zt, zt)
        return remote(prod.at[k, at, :, other], peer.at[k, at], dd_s.at[k, i], dd_r.at[k, i], {"tp": other})

    left, right, outs = (cott, tokt, tokt), (hid, gb, ub), (dg_ref, gg_ref, ug_ref)

    early = 2 * rows

    def tiles(e):
        for i in range(e * hz // zt, (e + 1) * hz // zt):
            for j in range(ff // nt):
                yield i, pl.ds(i * zt * zw, zt * zw), pl.ds(j * nt, nt), j == ff // nt - 1

    def first_sums(k, e):
        for i, lines, cols, _ in tiles(e):
            acc = jnp.dot(left[k][lines, :early], right[k][:early, cols], preferred_element_type=F32)
            prod[k, i * zt : (i + 1) * zt, :, :, :, cols] = acc.astype(BF16).reshape(zt, NY, 2, 32, nt)

    def weight_sums(k, e, begun):
        for i, lines, cols, last in tiles(e):
            at = (k, slice(i * zt, (i + 1) * zt), slice(None), slice(None), slice(None), cols)
            if begun:
                acc = jnp.dot(left[k][lines, early:], right[k][early:, cols], preferred_element_type=F32)
                acc += prod[at].reshape(zt * zw, nt).astype(F32)
            else:
                acc = jnp.dot(left[k][lines, :], right[k][:, cols], preferred_element_type=F32)
            prod[at] = acc.astype(BF16).reshape(zt, NY, 2, 32, nt)
            if last:
                pair(k, i).start()

    def pair_sum(k, e):
        for i in range(e * hz // zt, (e + 1) * hz // zt):
            pair(k, i).wait_recv()
        wa = WIDTH_A[k]

        def one(i, _):
            for j in range(NY):
                both = prod[k, i, j, t].astype(F32) + peer[k, i, j].astype(F32)
                both = both.astype(BF16)
                sa[k][i, j] = both[:, :wa]
                sb[k][i, j] = both[:, wa:]
            return 0

        lax.fori_loop(e * hz, (e + 1) * hz, one, 0)

    ly, lz = (2, 1), (4, 3)

    def sems(k, e, h, n):
        u = (k * 2 + e) * 2 + h
        return rs_s.at[u, n], rs_r.at[u, n]

    def go(way):
        return sgn if way == 0 else -sgn

    def a_y(k, e, way, step):
        m = step if way == 0 else 2
        at = pl.ds(e * hz, hz)
        dest = along_y((ly[way] - step) * go(way))
        return remote(sa[k].at[at, dest], ya[k].at[m, at], *sems(k, e, 0, m), dev_y(go(way)))

    hops = {"a": (4, 2), "b": (3, 1), "c": (1, 1), "d": (2, 2), "e": (-3, -2), "f": (-2, -1), "g": (-1, -1)}

    def a_z(k, e, name):
        m = "abcdefg".index(name)
        owner, target = hops[name]
        src = sa[k].at[place(along_z(owner * sgn)), y]
        return remote(src, za[k].at[m], *sems(k, e, 0, 3 + m), dev_z(target * sgn))

    def a_c(k, e, way, step):
        m = step if way == 0 else lz[0] + step
        src = sa[k].at[place(along_z((lz[way] - step) * go(way))), y]
        return remote(src, za[k].at[m], *sems(k, e, 0, 3 + m), dev_z(go(way)))

    def b_z(k, e, way, step):
        m = step if way == 0 else lz[0] + step
        src = sb[k].at[place(along_z((lz[way] - step) * go(way)))]
        return remote(src, zb[k].at[m], *sems(k, e, 1, m), dev_z(go(way)))

    y_steps = (1, -1, 2)

    def b_y(k, e, m):
        src = sb[k].at[place(z), along_y(y_steps[m])]
        return remote(src, yb[k].at[m], *sems(k, e, 1, 7 + m), dev_y(y_steps[m]))

    def added(ref, at, arrived):
        v = ref[at].astype(F32)
        for got in arrived:
            v += got.astype(F32)
        return v

    def a_chain(k, e, n):
        def run(rest_of):
            def go_on():
                for way in range(2):
                    if n >= lz[way] or (lz[way] - n) % 2 != rest_of:
                        continue
                    if n > 0:
                        a_c(k, e, way, n - 1).wait_recv()
                        at = (place(along_z((lz[way] - n) * go(way))), y)
                        got = za[k][n - 1 if way == 0 else lz[0] + n - 1]
                        sa[k][at] = added(sa[k], at, [got]).astype(BF16)
                    a_c(k, e, way, n).start()

            return go_on

        def end():
            a_c(k, e, 0, 3).wait_recv()
            a_c(k, e, 1, 2).wait_recv()
            v = added(sa[k], (place(z), y), [za[k][3], za[k][6]])
            outs[k][:, : WIDTH_A[k]] = v * scale

        if n < lz[0]:
            on_parity(e, run(0), run(1))
        else:
            on_parity(e, end)

    def a_stage(k, e, n):
        names = "abcdefg"
        if n <= 1:
            for way in range(2):
                if n >= ly[way]:
                    continue
                if n == 1:
                    a_y(k, e, way, 0).wait_recv()
                    at = along_y((ly[way] - 1) * go(way))
                    for i in range(e * hz, (e + 1) * hz):
                        sa[k][i, at] = added(sa[k], (i, at), [ya[k][0, i]]).astype(BF16)
                a_y(k, e, way, n).start()
        elif n == 2:
            a_y(k, e, 0, 1).wait_recv()
            a_y(k, e, 1, 0).wait_recv()
            for i in range(e * hz, (e + 1) * hz):
                sa[k][i, y] = added(sa[k], (i, y), [ya[k][1, i], ya[k][2, i]]).astype(BF16)
            if k in CHAINED:
                a_chain(k, e, 0)
                return

            def yes():
                for name in "af":
                    a_z(k, e, name).start()

            def no():
                for name in "ecb":
                    a_z(k, e, name).start()

            on_parity(e, yes, no)
        elif k in CHAINED:
            a_chain(k, e, n - 2)
        elif n == 3:

            def relay(one, two, step, out):
                a_z(k, e, one).wait_recv()
                a_z(k, e, two).wait_recv()
                at = (place(along_z(step * sgn)), y)
                got = [za[k][names.index(one)], za[k][names.index(two)]]
                sa[k][at] = added(sa[k], at, got).astype(BF16)
                a_z(k, e, out).start()

            on_parity(e, lambda: relay("a", "b", 2, "d"), lambda: relay("e", "f", -1, "g"))
        else:

            def end():
                for name in "cdg":
                    a_z(k, e, name).wait_recv()
                v = added(sa[k], (place(z), y), [za[k][names.index(c)] for c in "cdg"])
                outs[k][:, : WIDTH_A[k]] = v * scale

            on_parity(e, end)

    def b_sum(k, at, ms):
        for j in range(NY):
            sb[k][at, j] = added(sb[k], (at, j), [zb[k][m, j] for m in ms]).astype(BF16)

    def b_stage(k, e, n):
        if n <= 3:

            def step(way):
                if n > 0:
                    b_z(k, e, way, n - 1).wait_recv()
                    m = n - 1 if way == 0 else lz[0] + n - 1
                    b_sum(k, place(along_z((lz[way] - n) * go(way))), [m])
                b_z(k, e, way, n).start()

            def steps(rest_of):
                def run():
                    for way in range(2):
                        if n < lz[way] and (lz[way] - n) % 2 == rest_of:
                            step(way)

                return run

            on_parity(e, steps(0), steps(1))
        elif n == 4:

            def turn():
                b_z(k, e, 0, 3).wait_recv()
                b_z(k, e, 1, 2).wait_recv()
                b_sum(k, place(z), [3, 6])
                for m in range(3):
                    b_y(k, e, m).start()

            on_parity(e, turn)
        else:

            def end():
                for m in range(3):
                    b_y(k, e, m).wait_recv()
                v = added(sb[k], (place(z), y), [yb[k][m] for m in range(3)])
                outs[k][:, WIDTH_A[k] :] = v * scale

            on_parity(e, end)

    def stage(k, e, h, n):
        (a_stage, b_stage)[h](k, e, n)

    loads[0].wait()
    gather_out(0)
    loads[1].wait()
    loads[2].wait()
    forward(OWN)
    turn_weights()
    pass_on(0)
    for load in loads[3 : 3 + nz]:
        load.wait()
    gather_out(1)
    for load in loads[3 + nz :]:
        load.wait()
    hid_part(OWN)
    turned_cot(0, OWN)
    backward(OWN)
    turned_cot(1, OWN)
    input_part(OWN)
    gather_in(0, 0, 1)
    forward(PRV)
    gather_in(0, 1, 1)
    forward(NXT)
    gather_in(0, 0, 2)
    gather_in(0, 1, 2)
    forward(OPP)
    pass_on(1)
    gather_out(2)
    gather_in(1, 0, 1)
    hid_part(PRV)
    turned_cot(0, PRV)
    gather_in(1, 1, 1)
    hid_part(NXT)
    turned_cot(0, NXT)
    first_sums(0, 0)
    gather_in(1, 0, 2)
    gather_in(1, 1, 2)
    turned_cot(0, OPP)
    weight_sums(0, 0, True)
    pass_on(2)
    pair_sum(0, 0)
    stage(0, 0, 1, 0)
    stage(0, 0, 0, 0)
    gather_in(2, 0, 1)
    gather_in(2, 1, 1)
    hid_part(OPP)
    backward(NXT)
    turned_cot(1, NXT)
    first_sums(1, 0)
    first_sums(0, 1)
    backward(PRV)
    turned_cot(1, PRV)
    stage(0, 0, 1, 1)
    first_sums(1, 1)
    stage(0, 0, 0, 1)
    gather_in(2, 0, 2)
    gather_in(2, 1, 2)
    turned_cot(1, OPP)
    weight_sums(0, 1, True)
    backward(OPP)
    weight_sums(1, 0, True)
    pair_sum(0, 1)
    stage(0, 1, 1, 0)
    stage(0, 1, 0, 0)
    weight_sums(1, 1, True)
    pair_sum(1, 0)
    stage(1, 0, 1, 0)
    stage(1, 0, 0, 0)
    weight_sums(2, 0, False)
    pair_sum(1, 1)
    stage(1, 1, 1, 0)
    stage(0, 1, 1, 1)
    pair_sum(2, 0)
    stage(0, 0, 0, 2)
    stage(2, 0, 1, 0)
    stage(2, 0, 0, 0)
    weight_sums(2, 1, False)
    stage(1, 1, 0, 0)
    stage(1, 0, 1, 1)
    input_part(NXT)
    stage(1, 1, 1, 1)
    input_part(OPP)
    pair_sum(2, 1)
    stage(0, 0, 0, 3)
    stage(0, 0, 1, 2)
    x_start()
    stage(2, 1, 1, 0)
    stage(1, 0, 0, 1)
    stage(0, 1, 0, 1)
    stage(2, 0, 1, 1)
    stage(2, 1, 0, 0)
    stage(1, 1, 1, 2)
    input_part(PRV)
    stage(0, 1, 1, 2)
    stage(1, 1, 0, 1)
    stage(2, 1, 1, 1)
    x_direct()
    stage(0, 0, 1, 3)
    stage(1, 0, 1, 2)
    stage(2, 0, 1, 2)
    stage(0, 0, 0, 4)
    stage(1, 1, 1, 3)
    stage(0, 1, 0, 2)
    stage(2, 1, 1, 2)
    stage(1, 0, 0, 2)
    stage(2, 0, 0, 1)
    stage(1, 1, 0, 2)
    stage(1, 0, 1, 3)
    stage(2, 1, 0, 1)
    stage(0, 1, 1, 3)
    stage(2, 0, 1, 3)
    stage(0, 0, 1, 4)
    stage(2, 0, 0, 2)
    stage(1, 1, 1, 4)
    stage(1, 1, 0, 3)
    x_forward()
    stage(1, 0, 0, 3)
    stage(0, 1, 0, 3)
    stage(2, 1, 1, 3)
    stage(2, 1, 0, 2)
    stage(1, 0, 0, 4)
    stage(1, 0, 1, 4)
    stage(1, 1, 0, 4)
    stage(0, 1, 0, 4)
    stage(0, 0, 0, 5)
    stage(2, 0, 1, 4)
    stage(0, 1, 1, 4)
    stage(2, 0, 0, 3)
    stage(1, 1, 0, 5)
    stage(0, 1, 0, 5)
    stage(2, 1, 1, 4)
    stage(0, 0, 1, 5)
    stage(1, 1, 1, 5)
    stage(2, 1, 0, 3)
    stage(1, 0, 0, 5)
    x_finish()
    stage(0, 1, 0, 6)
    stage(0, 1, 1, 5)
    stage(1, 0, 0, 6)
    stage(2, 0, 1, 5)
    stage(2, 0, 0, 4)
    stage(1, 0, 1, 5)
    stage(2, 1, 1, 5)
    stage(1, 1, 0, 6)
    stage(0, 0, 0, 6)
    stage(2, 1, 0, 4)

    for a in range(3):
        for way in range(2):
            for k in range(3):
                gather(a, way, k).wait_send()
    for way in range(2):
        x_first(way).wait_send()
        x_second(way, True).wait_send()
        x_second(way, False).wait_send()
    for k in range(3):
        for i in range(nz // zt):
            pair(k, i).wait_send()
        for e in range(2):
            for way, step in ((0, 0), (0, 1), (1, 0)):
                a_y(k, e, way, step).wait_send()

    def sent(k, e, names, steps, direct):
        for name in () if k in CHAINED else names:
            a_z(k, e, name).wait_send()
        for way, step in steps:
            b_z(k, e, way, step).wait_send()
            if k in CHAINED:
                a_c(k, e, way, step).wait_send()
        for m in direct:
            b_y(k, e, m).wait_send()

    for e in range(2):

        def yes():
            for k in range(3):
                sent(k, e, "afd", ((0, 0), (0, 2), (1, 1)), range(3))

        def no():
            for k in range(3):
                sent(k, e, "bceg", ((0, 1), (0, 3), (1, 0), (1, 2)), ())

        on_parity(e, yes, no)


def written(*refs):
    n = (len(refs) - 1) // 2
    copies = [pltpu.make_async_copy(refs[k], refs[n + k], refs[-1].at[k]) for k in range(n)]
    for copy in copies:
        copy.start()
    for copy in copies:
        copy.wait()


def solution(mesh):
    n_rep = mesh.shape["rep"]
    nz = n_rep // NY
    nx = mesh.shape["fs"]
    cores = mesh.shape["tp"]

    def on_device(tokens, cotangent, gate_weight, up_weight, down_weight_t):
        rows, d = tokens.shape
        ff = gate_weight.shape[1]
        scale = float(rows * n_rep * nx * cores) ** (-0.5)
        lines = d // (n_rep * cores)
        wb = tuple(ff - w for w in WIDTH_A)
        shapes = (((rows, d), BF16),) + (((lines, ff), F32),) * 3
        vmem = pl.BlockSpec(memory_space=pltpu.VMEM)
        dma = pltpu.SemaphoreType.DMA
        results = pl.pallas_call(
            functools.partial(body, nz, scale),
            out_shape=tuple(pltpu.VMEM(*s) for s in shapes),
            in_specs=[pl.BlockSpec(memory_space=pl.ANY)] * 5,
            out_specs=(vmem,) * 4,
            scratch_shapes=[
                pltpu.VMEM((nx, rows, d), BF16),
                pltpu.VMEM((2, nx, rows, d // 2), BF16),
                pltpu.VMEM((d, nx * rows), BF16),
                pltpu.VMEM((d, nx * rows), BF16),
                pltpu.VMEM((d, ff), BF16),
                pltpu.VMEM((d, ff), BF16),
                pltpu.VMEM((d, ff), BF16),
                pltpu.VMEM((ff, d), BF16),
                pltpu.VMEM((ff, d), BF16),
                pltpu.VMEM((nx, rows, ff), F32),
                pltpu.VMEM((nx, rows, ff), F32),
                pltpu.VMEM((nx, rows, ff), F32),
                pltpu.VMEM((nx * rows, ff), BF16),
                pltpu.VMEM((nx * rows, ff), BF16),
                pltpu.VMEM((nx * rows, ff), BF16),
                pltpu.VMEM((nx, rows, d), BF16),
                pltpu.VMEM((2, rows // 2, d), BF16),
                pltpu.VMEM((2, rows, d), BF16),
                pltpu.VMEM((3, nz, NY, cores, lines, ff), BF16),
                pltpu.VMEM((3, nz, NY, lines, ff), BF16),
                *[pltpu.VMEM((nz, NY, lines, w), BF16) for w in WIDTH_A],
                *[pltpu.VMEM((nz, NY, lines, w), BF16) for w in wb],
                *[pltpu.VMEM((3, nz, lines, w), BF16) for w in WIDTH_A],
                *[pltpu.VMEM((7, lines, w), BF16) for w in WIDTH_A],
                *[pltpu.VMEM((7, NY, lines, w), BF16) for w in wb],
                *[pltpu.VMEM((3, lines, w), BF16) for w in wb],
                dma((3 + 2 * nz,)),
                dma((3, 2, 3)),
                dma((3, 2, 3)),
                dma((3, nz // 2)),
                dma((3, nz // 2)),
                dma((6,)),
                dma((6,)),
                dma((12, 10)),
                dma((12, 10)),
            ],
            compiler_params=pltpu.CompilerParams(
                collective_id=0, has_side_effects=True, vmem_limit_bytes=60 * 1024 * 1024
            ),
        )(tokens, cotangent, gate_weight, up_weight, down_weight_t)
        return pl.pallas_call(
            written,
            out_shape=tuple(jax.ShapeDtypeStruct(*s) for s in shapes),
            in_specs=[vmem] * 4,
            out_specs=(pl.BlockSpec(memory_space=pltpu.HBM),) * 4,
            scratch_shapes=[dma((4,))],
        )(*[pltpu.with_memory_space_constraint(r, pltpu.VMEM) for r in results])

    return jax.shard_map(
        on_device,
        mesh=mesh,
        in_specs=(
            P(("rep", "fs", "tp"), None),
            P(("rep", "fs", "tp"), None),
            P(None, "fs"),
            P(None, "fs"),
            P(None, "fs"),
        ),
        out_specs=(
            P(("rep", "fs", "tp"), None),
            P(("rep", "tp"), "fs"),
            P(("rep", "tp"), "fs"),
            P(("rep", "tp"), "fs"),
        ),
        check_vma=False,
    )
```

```python
import functools

import jax
import jax.numpy as jnp
from jax import lax
from jax.experimental import pallas as pl
from jax.experimental.pallas import tpu as pltpu
from jax.sharding import PartitionSpec as P

MESH = pl.DeviceIdType.MESH
F32 = jnp.float32
BF16 = jnp.bfloat16
NY = 4
WIDTH_A = (384, 384, 512)
CHAINED = ()
OWN, NXT, PRV, OPP = range(4)


def body(
    nz, scale, tok_hbm, cot_hbm, gw_hbm, uw_hbm, dw_hbm, ig_ref, gg_ref, ug_ref, dg_ref,
    tok, cot, tokt, cott, gw, uw, dw, gwt, uwt, gpre, upre, hpre, hid, gb, ub, part, xhalf, xfull,
    prod, peer, *rest,
):
    sa, sb, ya, za, zb, yb = (rest[3 * i : 3 * i + 3] for i in range(6))
    ld_sem, ag_s, ag_r, dd_s, dd_r, xs_s, xs_r, rs_s, rs_r = rest[18:]
    rep = lax.axis_index("rep")
    x = lax.axis_index("fs")
    t = lax.axis_index("tp")
    nx = 4
    rows = tok.shape[1]
    half = rows // 2
    d, ff = gw.shape
    hd = d // 2
    zw = d // nz
    hz = nz // 2
    z = rep // NY
    y = lax.rem(rep, NY)
    nxt, prv = lax.rem(x + 1, nx), lax.rem(x + nx - 1, nx)
    other = 1 - t
    sgn = 1 - 2 * t

    def along_y(step):
        return lax.rem(y + NY + step, NY)

    def along_z(step):
        return lax.rem(z + nz + step, nz)

    def place(zi):
        return zi % 2 * hz + zi // 2 if isinstance(zi, int) else lax.rem(zi, 2) * hz + zi // 2

    def dev_y(step):
        return {"rep": z * NY + along_y(step)}

    def dev_z(step):
        return {"rep": along_z(step) * NY + y}

    def on_parity(e, yes, no=None):
        mine = lax.rem(z, 2) == e
        pl.when(mine)(yes)
        if no is not None:
            pl.when(jnp.logical_not(mine))(no)

    parts = [(tok_hbm, tok.at[OWN]), (gw_hbm, gw), (uw_hbm, uw)]
    for zi in range(nz):
        cols = pl.ds(zi * zw, zw)
        parts.append((cot_hbm.at[:, cols], cot.at[zi % 2, OWN, :, pl.ds(zi // 2 * zw, zw)]))
    for zi in range(nz):
        parts.append((dw_hbm.at[pl.ds(zi * zw, zw), :], dw.at[pl.ds(place(zi) * zw, zw), :]))
    loads = [pltpu.make_async_copy(src, dst, ld_sem.at[k]) for k, (src, dst) in enumerate(parts)]
    for load in loads:
        load.start()

    barrier = pltpu.get_barrier_semaphore()
    peers = [{"fs": nxt}, {"fs": prv}, {"tp": other}]
    peers += [dev_y(s) for s in (1, -1, 2)] + [dev_z(s) for s in (1, -1, 2, -2)]
    for who in peers:
        pl.semaphore_signal(barrier, inc=1, device_id=who, device_id_type=MESH)
    pl.semaphore_wait(barrier, len(peers))

    def remote(src, dst, s, r, who):
        return pltpu.make_async_remote_copy(
            src_ref=src, dst_ref=dst, send_sem=s, recv_sem=r, device_id=who, device_id_type=MESH
        )

    bufs = (tok, cot.at[0], cot.at[1])
    to = ({"fs": nxt}, {"fs": prv})
    came = (PRV, NXT)

    def gather(a, way, k):
        h = way if k == 2 else (k if way == 0 else 1 - k)
        at = pl.ds(h * half, half)
        src, dst = (came[way], OPP) if k == 2 else (OWN, came[way])
        return remote(
            bufs[a].at[src, at, :], bufs[a].at[dst, at, :], ag_s.at[a, way, k], ag_r.at[a, way, k], to[way]
        )

    def gather_out(a):
        for k in range(2):
            for way in range(2):
                gather(a, way, k).start()

    def gather_in(a, way, k):
        gather(a, way, k).wait_recv()

    def pass_on(a):
        for way in range(2):
            gather_in(a, way, 0)
            gather(a, way, 2).start()

    nt = 256

    def rows_of(slot):
        return pl.ds(slot * rows, rows)

    def turned_cot(e, slot):
        cott[e * hd : (e + 1) * hd, rows_of(slot)] = cot[e, slot].T

    def turn_weights():
        def one(i, _):
            lines = pl.ds(pl.multiple_of(i * nt, nt), nt)
            gwt[:, lines] = gw[lines, :].T
            uwt[:, lines] = uw[lines, :].T
            return 0

        lax.fori_loop(0, d // nt, one, 0)

    def forward(slot):
        at = rows_of(slot)
        for i in range(ff // nt):
            cols = pl.ds(i * nt, nt)
            g = jnp.dot(tok[slot], gw[:, cols], preferred_element_type=F32)
            u = jnp.dot(tok[slot], uw[:, cols], preferred_element_type=F32)
            gpre[slot, :, cols] = g
            upre[slot, :, cols] = u
            hid[at, cols] = (g * jax.nn.sigmoid(g) * u).astype(BF16)
        for zi in range(nz):
            tokt[place(zi) * zw : (place(zi) + 1) * zw, at] = tok[slot, :, zi * zw : (zi + 1) * zw].T

    def hid_part(slot):
        for i in range(ff // nt):
            cols = pl.ds(i * nt, nt)
            hpre[slot, :, cols] = jnp.dot(cot[0, slot], dw[0:hd, cols], preferred_element_type=F32)

    def backward(slot):
        at = rows_of(slot)
        for i in range(ff // nt):
            cols = pl.ds(i * nt, nt)
            h = hpre[slot, :, cols] + jnp.dot(cot[1, slot], dw[hd:d, cols], preferred_element_type=F32)
            g = gpre[slot, :, cols]
            sig = jax.nn.sigmoid(g)
            gb[at, cols] = (h * upre[slot, :, cols] * sig * (1.0 + g * (1.0 - sig))).astype(BF16)
            ub[at, cols] = (h * (g * sig)).astype(BF16)

    def input_part(slot):
        at = rows_of(slot)
        for i in range(d // nt):
            cols = pl.ds(i * nt, nt)
            p = jnp.dot(gb[at, :], gwt[:, cols], preferred_element_type=F32)
            p += jnp.dot(ub[at, :], uwt[:, cols], preferred_element_type=F32)
            part[slot, :, cols] = p.astype(BF16)

    def x_first(way):
        return remote(
            part.at[OPP, pl.ds(way * half, half), :], xhalf.at[way], xs_s.at[way], xs_r.at[way], to[way]
        )

    def x_second(way, direct):
        at = pl.ds((1 - way if direct else way) * half, half)
        n = (4 if direct else 2) + way
        return remote(part.at[(NXT, PRV)[way], at, :], xfull.at[way, at, :], xs_s.at[n], xs_r.at[n], to[way])

    def x_direct():
        for way in range(2):
            x_second(way, True).start()

    def x_start():
        for way in range(2):
            x_first(way).start()

    def x_forward():
        for way in range(2):
            x_first(way).wait_recv()
            slot = (NXT, PRV)[way]
            for i in range(half // 16):
                at = pl.ds(way * half + i * 16, 16)
                got = xhalf[way, pl.ds(i * 16, 16), :].astype(F32)
                part[slot, at, :] = (part[slot, at, :].astype(F32) + got).astype(BF16)
            x_second(way, False).start()

    def x_finish():
        for way in range(2):
            x_second(way, True).wait_recv()
            x_second(way, False).wait_recv()

        def one(i, _):
            at = pl.ds(pl.multiple_of(i * 16, 16), 16)
            total = part[OWN, at, :].astype(F32) + xfull[0, at, :].astype(F32) + xfull[1, at, :].astype(F32)
            ig_ref[at, :] = total.astype(BF16)
            return 0

        lax.fori_loop(0, rows // 16, one, 0)

    zt = 2

    def pair(k, i):
        at = pl.ds(i * zt, zt)
        return remote(prod.at[k, at, :, other], peer.at[k, at], dd_s.at[k, i], dd_r.at[k, i], {"tp": other})

    left, right, outs = (cott, tokt, tokt), (hid, gb, ub), (dg_ref, gg_ref, ug_ref)

    early = 2 * rows

    def tiles(e):
        for i in range(e * hz // zt, (e + 1) * hz // zt):
            for j in range(ff // nt):
                yield i, pl.ds(i * zt * zw, zt * zw), pl.ds(j * nt, nt), j == ff // nt - 1

    def first_sums(k, e):
        for i, lines, cols, _ in tiles(e):
            acc = jnp.dot(left[k][lines, :early], right[k][:early, cols], preferred_element_type=F32)
            prod[k, i * zt : (i + 1) * zt, :, :, :, cols] = acc.astype(BF16).reshape(zt, NY, 2, 32, nt)

    def weight_sums(k, e, begun):
        for i, lines, cols, last in tiles(e):
            at = (k, slice(i * zt, (i + 1) * zt), slice(None), slice(None), slice(None), cols)
            if begun:
                acc = jnp.dot(left[k][lines, early:], right[k][early:, cols], preferred_element_type=F32)
                acc += prod[at].reshape(zt * zw, nt).astype(F32)
            else:
                acc = jnp.dot(left[k][lines, :], right[k][:, cols], preferred_element_type=F32)
            prod[at] = acc.astype(BF16).reshape(zt, NY, 2, 32, nt)
            if last:
                pair(k, i).start()

    def pair_sum(k, e):
        for i in range(e * hz // zt, (e + 1) * hz // zt):
            pair(k, i).wait_recv()
        wa = WIDTH_A[k]

        def one(i, _):
            for j in range(NY):
                both = prod[k, i, j, t].astype(F32) + peer[k, i, j].astype(F32)
                both = both.astype(BF16)
                sa[k][i, j] = both[:, :wa]
                sb[k][i, j] = both[:, wa:]
            return 0

        lax.fori_loop(e * hz, (e + 1) * hz, one, 0)

    ly, lz = (2, 1), (4, 3)

    def sems(k, e, h, n):
        u = (k * 2 + e) * 2 + h
        return rs_s.at[u, n], rs_r.at[u, n]

    def go(way):
        return sgn if way == 0 else -sgn

    def a_y(k, e, way, step):
        m = step if way == 0 else 2
        at = pl.ds(e * hz, hz)
        dest = along_y((ly[way] - step) * go(way))
        return remote(sa[k].at[at, dest], ya[k].at[m, at], *sems(k, e, 0, m), dev_y(go(way)))

    hops = {"a": (4, 2), "b": (3, 1), "c": (1, 1), "d": (2, 2), "e": (-3, -2), "f": (-2, -1), "g": (-1, -1)}

    def a_z(k, e, name):
        m = "abcdefg".index(name)
        owner, target = hops[name]
        src = sa[k].at[place(along_z(owner * sgn)), y]
        return remote(src, za[k].at[m], *sems(k, e, 0, 3 + m), dev_z(target * sgn))

    def a_c(k, e, way, step):
        m = step if way == 0 else lz[0] + step
        src = sa[k].at[place(along_z((lz[way] - step) * go(way))), y]
        return remote(src, za[k].at[m], *sems(k, e, 0, 3 + m), dev_z(go(way)))

    def b_z(k, e, way, step):
        m = step if way == 0 else lz[0] + step
        src = sb[k].at[place(along_z((lz[way] - step) * go(way)))]
        return remote(src, zb[k].at[m], *sems(k, e, 1, m), dev_z(go(way)))

    y_steps = (1, -1, 2)

    def b_y(k, e, m):
        src = sb[k].at[place(z), along_y(y_steps[m])]
        return remote(src, yb[k].at[m], *sems(k, e, 1, 7 + m), dev_y(y_steps[m]))

    def added(ref, at, arrived):
        v = ref[at].astype(F32)
        for got in arrived:
            v += got.astype(F32)
        return v

    def a_chain(k, e, n):
        def run(rest_of):
            def go_on():
                for way in range(2):
                    if n >= lz[way] or (lz[way] - n) % 2 != rest_of:
                        continue
                    if n > 0:
                        a_c(k, e, way, n - 1).wait_recv()
                        at = (place(along_z((lz[way] - n) * go(way))), y)
                        got = za[k][n - 1 if way == 0 else lz[0] + n - 1]
                        sa[k][at] = added(sa[k], at, [got]).astype(BF16)
                    a_c(k, e, way, n).start()

            return go_on

        def end():
            a_c(k, e, 0, 3).wait_recv()
            a_c(k, e, 1, 2).wait_recv()
            v = added(sa[k], (place(z), y), [za[k][3], za[k][6]])
            outs[k][:, : WIDTH_A[k]] = v * scale

        if n < lz[0]:
            on_parity(e, run(0), run(1))
        else:
            on_parity(e, end)

    def a_stage(k, e, n):
        names = "abcdefg"
        if n <= 1:
            for way in range(2):
                if n >= ly[way]:
                    continue
                if n == 1:
                    a_y(k, e, way, 0).wait_recv()
                    at = along_y((ly[way] - 1) * go(way))
                    for i in range(e * hz, (e + 1) * hz):
                        sa[k][i, at] = added(sa[k], (i, at), [ya[k][0, i]]).astype(BF16)
                a_y(k, e, way, n).start()
        elif n == 2:
            a_y(k, e, 0, 1).wait_recv()
            a_y(k, e, 1, 0).wait_recv()
            for i in range(e * hz, (e + 1) * hz):
                sa[k][i, y] = added(sa[k], (i, y), [ya[k][1, i], ya[k][2, i]]).astype(BF16)
            if k in CHAINED:
                a_chain(k, e, 0)
                return

            def yes():
                for name in "af":
                    a_z(k, e, name).start()

            def no():
                for name in "ecb":
                    a_z(k, e, name).start()

            on_parity(e, yes, no)
        elif k in CHAINED:
            a_chain(k, e, n - 2)
        elif n == 3:

            def relay(one, two, step, out):
                a_z(k, e, one).wait_recv()
                a_z(k, e, two).wait_recv()
                at = (place(along_z(step * sgn)), y)
                got = [za[k][names.index(one)], za[k][names.index(two)]]
                sa[k][at] = added(sa[k], at, got).astype(BF16)
                a_z(k, e, out).start()

            on_parity(e, lambda: relay("a", "b", 2, "d"), lambda: relay("e", "f", -1, "g"))
        else:

            def end():
                for name in "cdg":
                    a_z(k, e, name).wait_recv()
                v = added(sa[k], (place(z), y), [za[k][names.index(c)] for c in "cdg"])
                outs[k][:, : WIDTH_A[k]] = v * scale

            on_parity(e, end)

    def b_sum(k, at, ms):
        for j in range(NY):
            sb[k][at, j] = added(sb[k], (at, j), [zb[k][m, j] for m in ms]).astype(BF16)

    def b_stage(k, e, n):
        if n <= 3:

            def step(way):
                if n > 0:
                    b_z(k, e, way, n - 1).wait_recv()
                    m = n - 1 if way == 0 else lz[0] + n - 1
                    b_sum(k, place(along_z((lz[way] - n) * go(way))), [m])
                b_z(k, e, way, n).start()

            def steps(rest_of):
                def run():
                    for way in range(2):
                        if n < lz[way] and (lz[way] - n) % 2 == rest_of:
                            step(way)

                return run

            on_parity(e, steps(0), steps(1))
        elif n == 4:

            def turn():
                b_z(k, e, 0, 3).wait_recv()
                b_z(k, e, 1, 2).wait_recv()
                b_sum(k, place(z), [3, 6])
                for m in range(3):
                    b_y(k, e, m).start()

            on_parity(e, turn)
        else:

            def end():
                for m in range(3):
                    b_y(k, e, m).wait_recv()
                v = added(sb[k], (place(z), y), [yb[k][m] for m in range(3)])
                outs[k][:, WIDTH_A[k] :] = v * scale

            on_parity(e, end)

    def stage(k, e, h, n):
        (a_stage, b_stage)[h](k, e, n)

    loads[0].wait()
    gather_out(0)
    loads[1].wait()
    loads[2].wait()
    forward(OWN)
    turn_weights()
    pass_on(0)
    for load in loads[3 : 3 + nz]:
        load.wait()
    gather_out(1)
    for load in loads[3 + nz :]:
        load.wait()
    hid_part(OWN)
    turned_cot(0, OWN)
    backward(OWN)
    turned_cot(1, OWN)
    input_part(OWN)
    gather_in(0, 0, 1)
    forward(PRV)
    gather_in(0, 1, 1)
    forward(NXT)
    gather_in(0, 0, 2)
    gather_in(0, 1, 2)
    forward(OPP)
    pass_on(1)
    gather_out(2)
    gather_in(1, 0, 1)
    hid_part(PRV)
    turned_cot(0, PRV)
    gather_in(1, 1, 1)
    hid_part(NXT)
    turned_cot(0, NXT)
    first_sums(0, 0)
    gather_in(1, 0, 2)
    gather_in(1, 1, 2)
    turned_cot(0, OPP)
    weight_sums(0, 0, True)
    pass_on(2)
    pair_sum(0, 0)
    stage(0, 0, 0, 0)
    stage(0, 0, 1, 0)
    gather_in(2, 0, 1)
    gather_in(2, 1, 1)
    backward(NXT)
    turned_cot(1, NXT)
    backward(PRV)
    turned_cot(1, PRV)
    first_sums(1, 1)
    first_sums(1, 0)
    first_sums(0, 1)
    stage(0, 0, 1, 1)
    hid_part(OPP)
    gather_in(2, 0, 2)
    gather_in(2, 1, 2)
    turned_cot(1, OPP)
    weight_sums(0, 1, True)
    backward(OPP)
    stage(0, 0, 0, 1)
    weight_sums(1, 0, True)
    pair_sum(0, 1)
    stage(0, 1, 0, 0)
    stage(0, 1, 1, 0)
    weight_sums(1, 1, True)
    stage(0, 0, 1, 2)
    pair_sum(1, 0)
    stage(1, 0, 0, 0)
    stage(1, 0, 1, 0)
    weight_sums(2, 0, False)
    pair_sum(1, 1)
    stage(1, 1, 1, 0)
    stage(0, 1, 1, 1)
    pair_sum(2, 0)
    stage(1, 1, 0, 0)
    stage(0, 0, 0, 2)
    weight_sums(2, 1, False)
    stage(2, 0, 1, 0)
    stage(2, 0, 0, 0)
    input_part(OPP)
    stage(1, 0, 1, 1)
    stage(0, 1, 0, 1)
    pair_sum(2, 1)
    stage(1, 1, 1, 1)
    stage(1, 0, 0, 1)
    stage(2, 1, 1, 0)
    input_part(PRV)
    input_part(NXT)
    stage(0, 1, 1, 2)
    stage(2, 1, 0, 0)
    stage(0, 0, 0, 3)
    x_start()
    stage(2, 0, 1, 1)
    stage(1, 0, 1, 2)
    stage(1, 1, 0, 1)
    stage(2, 1, 1, 1)
    stage(0, 1, 0, 2)
    stage(0, 0, 1, 3)
    stage(2, 0, 0, 1)
    stage(1, 1, 1, 2)
    stage(2, 0, 1, 2)
    stage(2, 1, 1, 2)
    stage(1, 0, 1, 3)
    x_direct()
    stage(0, 0, 0, 4)
    stage(0, 1, 1, 3)
    stage(2, 1, 0, 1)
    stage(1, 1, 0, 2)
    stage(2, 0, 0, 2)
    stage(0, 0, 1, 4)
    stage(1, 0, 0, 2)
    stage(2, 1, 1, 3)
    stage(0, 1, 1, 4)
    stage(1, 1, 1, 3)
    stage(2, 1, 0, 2)
    stage(2, 0, 1, 3)
    x_forward()
    stage(2, 1, 1, 4)
    stage(2, 0, 0, 3)
    stage(1, 1, 0, 3)
    stage(0, 1, 0, 3)
    stage(0, 1, 1, 5)
    stage(1, 1, 1, 4)
    stage(1, 0, 1, 4)
    stage(1, 0, 0, 3)
    stage(2, 1, 0, 3)
    stage(1, 1, 0, 4)
    stage(2, 0, 1, 4)
    x_finish()
    stage(1, 0, 0, 4)
    stage(0, 1, 0, 4)
    stage(2, 0, 0, 4)
    stage(1, 0, 1, 5)
    stage(2, 0, 1, 5)
    stage(1, 1, 1, 5)
    stage(0, 0, 1, 5)
    stage(2, 1, 1, 5)
    stage(2, 1, 0, 4)

    for a in range(3):
        for way in range(2):
            for k in range(3):
                gather(a, way, k).wait_send()
    for way in range(2):
        x_first(way).wait_send()
        x_second(way, True).wait_send()
        x_second(way, False).wait_send()
    for k in range(3):
        for i in range(nz // zt):
            pair(k, i).wait_send()
        for e in range(2):
            for way, step in ((0, 0), (0, 1), (1, 0)):
                a_y(k, e, way, step).wait_send()

    def sent(k, e, names, steps, direct):
        for name in () if k in CHAINED else names:
            a_z(k, e, name).wait_send()
        for way, step in steps:
            b_z(k, e, way, step).wait_send()
            if k in CHAINED:
                a_c(k, e, way, step).wait_send()
        for m in direct:
            b_y(k, e, m).wait_send()

    for e in range(2):

        def yes():
            for k in range(3):
                sent(k, e, "afd", ((0, 0), (0, 2), (1, 1)), range(3))

        def no():
            for k in range(3):
                sent(k, e, "bceg", ((0, 1), (0, 3), (1, 0), (1, 2)), ())

        on_parity(e, yes, no)


def written(*refs):
    n = (len(refs) - 1) // 2
    copies = [pltpu.make_async_copy(refs[k], refs[n + k], refs[-1].at[k]) for k in range(n)]
    for copy in copies:
        copy.start()
    for copy in copies:
        copy.wait()


def solution(mesh):
    n_rep = mesh.shape["rep"]
    nz = n_rep // NY
    nx = mesh.shape["fs"]
    cores = mesh.shape["tp"]

    def on_device(tokens, cotangent, gate_weight, up_weight, down_weight_t):
        rows, d = tokens.shape
        ff = gate_weight.shape[1]
        scale = float(rows * n_rep * nx * cores) ** (-0.5)
        lines = d // (n_rep * cores)
        wb = tuple(ff - w for w in WIDTH_A)
        shapes = (((rows, d), BF16),) + (((lines, ff), F32),) * 3
        vmem = pl.BlockSpec(memory_space=pltpu.VMEM)
        dma = pltpu.SemaphoreType.DMA
        results = pl.pallas_call(
            functools.partial(body, nz, scale),
            out_shape=tuple(pltpu.VMEM(*s) for s in shapes),
            in_specs=[pl.BlockSpec(memory_space=pl.ANY)] * 5,
            out_specs=(vmem,) * 4,
            scratch_shapes=[
                pltpu.VMEM((nx, rows, d), BF16),
                pltpu.VMEM((2, nx, rows, d // 2), BF16),
                pltpu.VMEM((d, nx * rows), BF16),
                pltpu.VMEM((d, nx * rows), BF16),
                pltpu.VMEM((d, ff), BF16),
                pltpu.VMEM((d, ff), BF16),
                pltpu.VMEM((d, ff), BF16),
                pltpu.VMEM((ff, d), BF16),
                pltpu.VMEM((ff, d), BF16),
                pltpu.VMEM((nx, rows, ff), F32),
                pltpu.VMEM((nx, rows, ff), F32),
                pltpu.VMEM((nx, rows, ff), F32),
                pltpu.VMEM((nx * rows, ff), BF16),
                pltpu.VMEM((nx * rows, ff), BF16),
                pltpu.VMEM((nx * rows, ff), BF16),
                pltpu.VMEM((nx, rows, d), BF16),
                pltpu.VMEM((2, rows // 2, d), BF16),
                pltpu.VMEM((2, rows, d), BF16),
                pltpu.VMEM((3, nz, NY, cores, lines, ff), BF16),
                pltpu.VMEM((3, nz, NY, lines, ff), BF16),
                *[pltpu.VMEM((nz, NY, lines, w), BF16) for w in WIDTH_A],
                *[pltpu.VMEM((nz, NY, lines, w), BF16) for w in wb],
                *[pltpu.VMEM((3, nz, lines, w), BF16) for w in WIDTH_A],
                *[pltpu.VMEM((7, lines, w), BF16) for w in WIDTH_A],
                *[pltpu.VMEM((7, NY, lines, w), BF16) for w in wb],
                *[pltpu.VMEM((3, lines, w), BF16) for w in wb],
                dma((3 + 2 * nz,)),
                dma((3, 2, 3)),
                dma((3, 2, 3)),
                dma((3, nz // 2)),
                dma((3, nz // 2)),
                dma((6,)),
                dma((6,)),
                dma((12, 10)),
                dma((12, 10)),
            ],
            compiler_params=pltpu.CompilerParams(
                collective_id=0, has_side_effects=True, vmem_limit_bytes=60 * 1024 * 1024
            ),
        )(tokens, cotangent, gate_weight, up_weight, down_weight_t)
        return pl.pallas_call(
            written,
            out_shape=tuple(jax.ShapeDtypeStruct(*s) for s in shapes),
            in_specs=[vmem] * 4,
            out_specs=(pl.BlockSpec(memory_space=pltpu.HBM),) * 4,
            scratch_shapes=[dma((4,))],
        )(*[pltpu.with_memory_space_constraint(r, pltpu.VMEM) for r in results])

    return jax.shard_map(
        on_device,
        mesh=mesh,
        in_specs=(
            P(("rep", "fs", "tp"), None),
            P(("rep", "fs", "tp"), None),
            P(None, "fs"),
            P(None, "fs"),
            P(None, "fs"),
        ),
        out_specs=(
            P(("rep", "fs", "tp"), None),
            P(("rep", "tp"), "fs"),
            P(("rep", "tp"), "fs"),
            P(("rep", "tp"), "fs"),
        ),
        check_vma=False,
    )
```

```python
import functools

import jax
import jax.numpy as jnp
from jax import lax
from jax.experimental import pallas as pl
from jax.experimental.pallas import tpu as pltpu
from jax.sharding import PartitionSpec as P

MESH = pl.DeviceIdType.MESH
F32 = jnp.float32
BF16 = jnp.bfloat16
NY = 4
WIDTH_A = (384, 384, 640)
CHAINED = ()
OWN, NXT, PRV, OPP = range(4)


def body(
    nz, scale, tok_hbm, cot_hbm, gw_hbm, uw_hbm, dw_hbm, ig_ref, gg_ref, ug_ref, dg_ref,
    tok, cot, tokt, cott, gw, uw, dw, gwt, uwt, gpre, upre, hpre, hid, gb, ub, part, xhalf, xfull,
    prod, peer, *rest,
):
    sa, sb, ya, za, zb, yb = (rest[3 * i : 3 * i + 3] for i in range(6))
    ld_sem, ag_s, ag_r, dd_s, dd_r, xs_s, xs_r, rs_s, rs_r = rest[18:]
    rep = lax.axis_index("rep")
    x = lax.axis_index("fs")
    t = lax.axis_index("tp")
    nx = 4
    rows = tok.shape[1]
    half = rows // 2
    d, ff = gw.shape
    hd = d // 2
    zw = d // nz
    hz = nz // 2
    z = rep // NY
    y = lax.rem(rep, NY)
    nxt, prv = lax.rem(x + 1, nx), lax.rem(x + nx - 1, nx)
    other = 1 - t
    sgn = 1 - 2 * t

    def along_y(step):
        return lax.rem(y + NY + step, NY)

    def along_z(step):
        return lax.rem(z + nz + step, nz)

    def place(zi):
        return zi % 2 * hz + zi // 2 if isinstance(zi, int) else lax.rem(zi, 2) * hz + zi // 2

    def dev_y(step):
        return {"rep": z * NY + along_y(step)}

    def dev_z(step):
        return {"rep": along_z(step) * NY + y}

    def on_parity(e, yes, no=None):
        mine = lax.rem(z, 2) == e
        pl.when(mine)(yes)
        if no is not None:
            pl.when(jnp.logical_not(mine))(no)

    parts = [(tok_hbm, tok.at[OWN]), (gw_hbm, gw), (uw_hbm, uw)]
    for zi in range(nz):
        cols = pl.ds(zi * zw, zw)
        parts.append((cot_hbm.at[:, cols], cot.at[zi % 2, OWN, :, pl.ds(zi // 2 * zw, zw)]))
    for zi in range(nz):
        parts.append((dw_hbm.at[pl.ds(zi * zw, zw), :], dw.at[pl.ds(place(zi) * zw, zw), :]))
    loads = [pltpu.make_async_copy(src, dst, ld_sem.at[k]) for k, (src, dst) in enumerate(parts)]
    for load in loads:
        load.start()

    barrier = pltpu.get_barrier_semaphore()
    peers = [{"fs": nxt}, {"fs": prv}, {"tp": other}]
    peers += [dev_y(s) for s in (1, -1, 2)] + [dev_z(s) for s in (1, -1, 2, -2)]
    for who in peers:
        pl.semaphore_signal(barrier, inc=1, device_id=who, device_id_type=MESH)
    pl.semaphore_wait(barrier, len(peers))

    def remote(src, dst, s, r, who):
        return pltpu.make_async_remote_copy(
            src_ref=src, dst_ref=dst, send_sem=s, recv_sem=r, device_id=who, device_id_type=MESH
        )

    bufs = (tok, cot.at[0], cot.at[1])
    to = ({"fs": nxt}, {"fs": prv})
    came = (PRV, NXT)

    def gather(a, way, k):
        h = way if k == 2 else (k if way == 0 else 1 - k)
        at = pl.ds(h * half, half)
        src, dst = (came[way], OPP) if k == 2 else (OWN, came[way])
        return remote(
            bufs[a].at[src, at, :], bufs[a].at[dst, at, :], ag_s.at[a, way, k], ag_r.at[a, way, k], to[way]
        )

    def gather_out(a):
        for k in range(2):
            for way in range(2):
                gather(a, way, k).start()

    def gather_in(a, way, k):
        gather(a, way, k).wait_recv()

    def pass_on(a):
        for way in range(2):
            gather_in(a, way, 0)
            gather(a, way, 2).start()

    nt = 256

    def rows_of(slot):
        return pl.ds(slot * rows, rows)

    def turned_cot(e, slot):
        cott[e * hd : (e + 1) * hd, rows_of(slot)] = cot[e, slot].T

    def turn_weights():
        def one(i, _):
            lines = pl.ds(pl.multiple_of(i * nt, nt), nt)
            gwt[:, lines] = gw[lines, :].T
            uwt[:, lines] = uw[lines, :].T
            return 0

        lax.fori_loop(0, d // nt, one, 0)

    def forward(slot):
        at = rows_of(slot)
        for i in range(ff // nt):
            cols = pl.ds(i * nt, nt)
            g = jnp.dot(tok[slot], gw[:, cols], preferred_element_type=F32)
            u = jnp.dot(tok[slot], uw[:, cols], preferred_element_type=F32)
            gpre[slot, :, cols] = g
            upre[slot, :, cols] = u
            hid[at, cols] = (g * jax.nn.sigmoid(g) * u).astype(BF16)
        for zi in range(nz):
            tokt[place(zi) * zw : (place(zi) + 1) * zw, at] = tok[slot, :, zi * zw : (zi + 1) * zw].T

    def hid_part(slot):
        for i in range(ff // nt):
            cols = pl.ds(i * nt, nt)
            hpre[slot, :, cols] = jnp.dot(cot[0, slot], dw[0:hd, cols], preferred_element_type=F32)

    def backward(slot):
        at = rows_of(slot)
        for i in range(ff // nt):
            cols = pl.ds(i * nt, nt)
            h = hpre[slot, :, cols] + jnp.dot(cot[1, slot], dw[hd:d, cols], preferred_element_type=F32)
            g = gpre[slot, :, cols]
            sig = jax.nn.sigmoid(g)
            gb[at, cols] = (h * upre[slot, :, cols] * sig * (1.0 + g * (1.0 - sig))).astype(BF16)
            ub[at, cols] = (h * (g * sig)).astype(BF16)

    def input_part(slot):
        at = rows_of(slot)
        for i in range(d // nt):
            cols = pl.ds(i * nt, nt)
            p = jnp.dot(gb[at, :], gwt[:, cols], preferred_element_type=F32)
            p += jnp.dot(ub[at, :], uwt[:, cols], preferred_element_type=F32)
            part[slot, :, cols] = p.astype(BF16)

    def x_first(way):
        return remote(
            part.at[OPP, pl.ds(way * half, half), :], xhalf.at[way], xs_s.at[way], xs_r.at[way], to[way]
        )

    def x_second(way, direct):
        at = pl.ds((1 - way if direct else way) * half, half)
        n = (4 if direct else 2) + way
        return remote(part.at[(NXT, PRV)[way], at, :], xfull.at[way, at, :], xs_s.at[n], xs_r.at[n], to[way])

    def x_direct():
        for way in range(2):
            x_second(way, True).start()

    def x_start():
        for way in range(2):
            x_first(way).start()

    def x_forward():
        for way in range(2):
            x_first(way).wait_recv()
            slot = (NXT, PRV)[way]
            for i in range(half // 16):
                at = pl.ds(way * half + i * 16, 16)
                got = xhalf[way, pl.ds(i * 16, 16), :].astype(F32)
                part[slot, at, :] = (part[slot, at, :].astype(F32) + got).astype(BF16)
            x_second(way, False).start()

    def x_finish():
        for way in range(2):
            x_second(way, True).wait_recv()
            x_second(way, False).wait_recv()

        def one(i, _):
            at = pl.ds(pl.multiple_of(i * 16, 16), 16)
            total = part[OWN, at, :].astype(F32) + xfull[0, at, :].astype(F32) + xfull[1, at, :].astype(F32)
            ig_ref[at, :] = total.astype(BF16)
            return 0

        lax.fori_loop(0, rows // 16, one, 0)

    zt = 2

    def pair(k, i):
        at = pl.ds(i * zt, zt)
        return remote(prod.at[k, at, :, other], peer.at[k, at], dd_s.at[k, i], dd_r.at[k, i], {"tp": other})

    left, right, outs = (cott, tokt, tokt), (hid, gb, ub), (dg_ref, gg_ref, ug_ref)

    early = 2 * rows

    def tiles(e):
        for i in range(e * hz // zt, (e + 1) * hz // zt):
            for j in range(ff // nt):
                yield i, pl.ds(i * zt * zw, zt * zw), pl.ds(j * nt, nt), j == ff // nt - 1

    def first_sums(k, e):
        for i, lines, cols, _ in tiles(e):
            acc = jnp.dot(left[k][lines, :early], right[k][:early, cols], preferred_element_type=F32)
            prod[k, i * zt : (i + 1) * zt, :, :, :, cols] = acc.astype(BF16).reshape(zt, NY, 2, 32, nt)

    def weight_sums(k, e, begun):
        for i, lines, cols, last in tiles(e):
            at = (k, slice(i * zt, (i + 1) * zt), slice(None), slice(None), slice(None), cols)
            if begun:
                acc = jnp.dot(left[k][lines, early:], right[k][early:, cols], preferred_element_type=F32)
                acc += prod[at].reshape(zt * zw, nt).astype(F32)
            else:
                acc = jnp.dot(left[k][lines, :], right[k][:, cols], preferred_element_type=F32)
            prod[at] = acc.astype(BF16).reshape(zt, NY, 2, 32, nt)
            if last:
                pair(k, i).start()

    def pair_sum(k, e):
        for i in range(e * hz // zt, (e + 1) * hz // zt):
            pair(k, i).wait_recv()
        wa = WIDTH_A[k]

        def one(i, _):
            for j in range(NY):
                both = prod[k, i, j, t].astype(F32) + peer[k, i, j].astype(F32)
                both = both.astype(BF16)
                sa[k][i, j] = both[:, :wa]
                sb[k][i, j] = both[:, wa:]
            return 0

        lax.fori_loop(e * hz, (e + 1) * hz, one, 0)

    ly, lz = (2, 1), (4, 3)

    def sems(k, e, h, n):
        u = (k * 2 + e) * 2 + h
        return rs_s.at[u, n], rs_r.at[u, n]

    def go(way):
        return sgn if way == 0 else -sgn

    def a_y(k, e, way, step):
        m = step if way == 0 else 2
        at = pl.ds(e * hz, hz)
        dest = along_y((ly[way] - step) * go(way))
        return remote(sa[k].at[at, dest], ya[k].at[m, at], *sems(k, e, 0, m), dev_y(go(way)))

    hops = {"a": (4, 2), "b": (3, 1), "c": (1, 1), "d": (2, 2), "e": (-3, -2), "f": (-2, -1), "g": (-1, -1)}

    def a_z(k, e, name):
        m = "abcdefg".index(name)
        owner, target = hops[name]
        src = sa[k].at[place(along_z(owner * sgn)), y]
        return remote(src, za[k].at[m], *sems(k, e, 0, 3 + m), dev_z(target * sgn))

    def a_c(k, e, way, step):
        m = step if way == 0 else lz[0] + step
        src = sa[k].at[place(along_z((lz[way] - step) * go(way))), y]
        return remote(src, za[k].at[m], *sems(k, e, 0, 3 + m), dev_z(go(way)))

    def b_z(k, e, way, step):
        m = step if way == 0 else lz[0] + step
        src = sb[k].at[place(along_z((lz[way] - step) * go(way)))]
        return remote(src, zb[k].at[m], *sems(k, e, 1, m), dev_z(go(way)))

    y_steps = (1, -1, 2)

    def b_y(k, e, m):
        src = sb[k].at[place(z), along_y(y_steps[m])]
        return remote(src, yb[k].at[m], *sems(k, e, 1, 7 + m), dev_y(y_steps[m]))

    def added(ref, at, arrived):
        v = ref[at].astype(F32)
        for got in arrived:
            v += got.astype(F32)
        return v

    def a_chain(k, e, n):
        def run(rest_of):
            def go_on():
                for way in range(2):
                    if n >= lz[way] or (lz[way] - n) % 2 != rest_of:
                        continue
                    if n > 0:
                        a_c(k, e, way, n - 1).wait_recv()
                        at = (place(along_z((lz[way] - n) * go(way))), y)
                        got = za[k][n - 1 if way == 0 else lz[0] + n - 1]
                        sa[k][at] = added(sa[k], at, [got]).astype(BF16)
                    a_c(k, e, way, n).start()

            return go_on

        def end():
            a_c(k, e, 0, 3).wait_recv()
            a_c(k, e, 1, 2).wait_recv()
            v = added(sa[k], (place(z), y), [za[k][3], za[k][6]])
            outs[k][:, : WIDTH_A[k]] = v * scale

        if n < lz[0]:
            on_parity(e, run(0), run(1))
        else:
            on_parity(e, end)

    def a_stage(k, e, n):
        names = "abcdefg"
        if n <= 1:
            for way in range(2):
                if n >= ly[way]:
                    continue
                if n == 1:
                    a_y(k, e, way, 0).wait_recv()
                    at = along_y((ly[way] - 1) * go(way))
                    for i in range(e * hz, (e + 1) * hz):
                        sa[k][i, at] = added(sa[k], (i, at), [ya[k][0, i]]).astype(BF16)
                a_y(k, e, way, n).start()
        elif n == 2:
            a_y(k, e, 0, 1).wait_recv()
            a_y(k, e, 1, 0).wait_recv()
            for i in range(e * hz, (e + 1) * hz):
                sa[k][i, y] = added(sa[k], (i, y), [ya[k][1, i], ya[k][2, i]]).astype(BF16)
            if k in CHAINED:
                a_chain(k, e, 0)
                return

            def yes():
                for name in "af":
                    a_z(k, e, name).start()

            def no():
                for name in "ecb":
                    a_z(k, e, name).start()

            on_parity(e, yes, no)
        elif k in CHAINED:
            a_chain(k, e, n - 2)
        elif n == 3:

            def relay(one, two, step, out):
                a_z(k, e, one).wait_recv()
                a_z(k, e, two).wait_recv()
                at = (place(along_z(step * sgn)), y)
                got = [za[k][names.index(one)], za[k][names.index(two)]]
                sa[k][at] = added(sa[k], at, got).astype(BF16)
                a_z(k, e, out).start()

            on_parity(e, lambda: relay("a", "b", 2, "d"), lambda: relay("e", "f", -1, "g"))
        else:

            def end():
                for name in "cdg":
                    a_z(k, e, name).wait_recv()
                v = added(sa[k], (place(z), y), [za[k][names.index(c)] for c in "cdg"])
                outs[k][:, : WIDTH_A[k]] = v * scale

            on_parity(e, end)

    def b_sum(k, at, ms):
        for j in range(NY):
            sb[k][at, j] = added(sb[k], (at, j), [zb[k][m, j] for m in ms]).astype(BF16)

    def b_stage(k, e, n):
        if n <= 3:

            def step(way):
                if n > 0:
                    b_z(k, e, way, n - 1).wait_recv()
                    m = n - 1 if way == 0 else lz[0] + n - 1
                    b_sum(k, place(along_z((lz[way] - n) * go(way))), [m])
                b_z(k, e, way, n).start()

            def steps(rest_of):
                def run():
                    for way in range(2):
                        if n < lz[way] and (lz[way] - n) % 2 == rest_of:
                            step(way)

                return run

            on_parity(e, steps(0), steps(1))
        elif n == 4:

            def turn():
                b_z(k, e, 0, 3).wait_recv()
                b_z(k, e, 1, 2).wait_recv()
                b_sum(k, place(z), [3, 6])
                for m in range(3):
                    b_y(k, e, m).start()

            on_parity(e, turn)
        else:

            def end():
                for m in range(3):
                    b_y(k, e, m).wait_recv()
                v = added(sb[k], (place(z), y), [yb[k][m] for m in range(3)])
                outs[k][:, WIDTH_A[k] :] = v * scale

            on_parity(e, end)

    def stage(k, e, h, n):
        (a_stage, b_stage)[h](k, e, n)

    loads[0].wait()
    gather_out(0)
    loads[1].wait()
    loads[2].wait()
    forward(OWN)
    turn_weights()
    pass_on(0)
    for load in loads[3 : 3 + nz]:
        load.wait()
    gather_out(1)
    for load in loads[3 + nz :]:
        load.wait()
    hid_part(OWN)
    turned_cot(0, OWN)
    backward(OWN)
    turned_cot(1, OWN)
    input_part(OWN)
    gather_in(0, 0, 1)
    forward(PRV)
    gather_in(0, 1, 1)
    forward(NXT)
    gather_in(0, 0, 2)
    gather_in(0, 1, 2)
    forward(OPP)
    pass_on(1)
    gather_out(2)
    gather_in(1, 0, 1)
    hid_part(PRV)
    turned_cot(0, PRV)
    gather_in(1, 1, 1)
    hid_part(NXT)
    turned_cot(0, NXT)
    first_sums(0, 0)
    gather_in(1, 0, 2)
    gather_in(1, 1, 2)
    turned_cot(0, OPP)
    weight_sums(0, 0, True)
    pass_on(2)
    pair_sum(0, 0)
    stage(0, 0, 0, 0)
    stage(0, 0, 1, 0)
    gather_in(2, 0, 1)
    gather_in(2, 1, 1)
    backward(NXT)
    turned_cot(1, NXT)
    backward(PRV)
    turned_cot(1, PRV)
    first_sums(0, 1)
    first_sums(1, 0)
    first_sums(1, 1)
    hid_part(OPP)
    stage(0, 0, 1, 1)
    gather_in(2, 0, 2)
    gather_in(2, 1, 2)
    turned_cot(1, OPP)
    weight_sums(0, 1, True)
    backward(OPP)
    stage(0, 0, 0, 1)
    weight_sums(1, 0, True)
    pair_sum(0, 1)
    stage(0, 1, 0, 0)
    stage(0, 1, 1, 0)
    weight_sums(1, 1, True)
    pair_sum(1, 0)
    stage(1, 0, 1, 0)
    stage(1, 0, 0, 0)
    stage(0, 0, 1, 2)
    weight_sums(2, 0, False)
    pair_sum(1, 1)
    stage(1, 1, 0, 0)
    stage(1, 1, 1, 0)
    weight_sums(2, 1, False)
    stage(0, 0, 0, 2)
    stage(0, 1, 1, 1)
    pair_sum(2, 0)
    input_part(OPP)
    stage(2, 0, 1, 0)
    stage(2, 0, 0, 0)
    stage(1, 1, 1, 1)
    pair_sum(2, 1)
    stage(1, 0, 1, 1)
    stage(0, 0, 1, 3)
    x_start()
    stage(1, 1, 0, 1)
    stage(2, 1, 1, 0)
    stage(2, 0, 1, 1)
    stage(0, 1, 0, 1)
    stage(0, 1, 1, 2)
    input_part(PRV)
    stage(2, 1, 0, 0)
    stage(1, 0, 0, 1)
    input_part(NXT)
    x_direct()
    stage(1, 0, 1, 2)
    stage(0, 0, 0, 3)
    stage(1, 1, 1, 2)
    stage(2, 1, 1, 1)
    stage(2, 0, 1, 2)
    stage(2, 0, 0, 1)
    stage(1, 1, 0, 2)
    stage(0, 1, 1, 3)
    stage(1, 0, 1, 3)
    stage(0, 1, 0, 2)
    x_forward()
    stage(2, 1, 1, 2)
    stage(2, 1, 0, 1)
    stage(1, 1, 1, 3)
    stage(2, 0, 1, 3)
    stage(1, 0, 0, 2)
    stage(2, 0, 0, 2)
    stage(1, 0, 1, 4)
    stage(2, 1, 1, 3)
    stage(2, 1, 0, 2)
    stage(0, 1, 0, 3)
    stage(2, 1, 1, 4)
    stage(0, 1, 1, 4)
    stage(1, 0, 1, 5)
    stage(2, 0, 0, 3)
    stage(1, 1, 1, 4)
    stage(1, 1, 0, 3)
    stage(0, 0, 1, 4)
    stage(1, 0, 0, 3)
    stage(2, 0, 1, 4)
    stage(2, 1, 0, 3)
    stage(2, 1, 1, 5)
    x_finish()
    stage(0, 0, 0, 4)
    stage(2, 0, 0, 4)
    stage(2, 0, 1, 5)
    stage(0, 0, 1, 5)
    stage(1, 1, 1, 5)
    stage(1, 1, 0, 4)
    stage(1, 0, 0, 4)
    stage(0, 1, 1, 5)
    stage(0, 1, 0, 4)
    stage(2, 1, 0, 4)

    for a in range(3):
        for way in range(2):
            for k in range(3):
                gather(a, way, k).wait_send()
    for way in range(2):
        x_first(way).wait_send()
        x_second(way, True).wait_send()
        x_second(way, False).wait_send()
    for k in range(3):
        for i in range(nz // zt):
            pair(k, i).wait_send()
        for e in range(2):
            for way, step in ((0, 0), (0, 1), (1, 0)):
                a_y(k, e, way, step).wait_send()

    def sent(k, e, names, steps, direct):
        for name in () if k in CHAINED else names:
            a_z(k, e, name).wait_send()
        for way, step in steps:
            b_z(k, e, way, step).wait_send()
            if k in CHAINED:
                a_c(k, e, way, step).wait_send()
        for m in direct:
            b_y(k, e, m).wait_send()

    for e in range(2):

        def yes():
            for k in range(3):
                sent(k, e, "afd", ((0, 0), (0, 2), (1, 1)), range(3))

        def no():
            for k in range(3):
                sent(k, e, "bceg", ((0, 1), (0, 3), (1, 0), (1, 2)), ())

        on_parity(e, yes, no)


def written(*refs):
    n = (len(refs) - 1) // 2
    copies = [pltpu.make_async_copy(refs[k], refs[n + k], refs[-1].at[k]) for k in range(n)]
    for copy in copies:
        copy.start()
    for copy in copies:
        copy.wait()


def solution(mesh):
    n_rep = mesh.shape["rep"]
    nz = n_rep // NY
    nx = mesh.shape["fs"]
    cores = mesh.shape["tp"]

    def on_device(tokens, cotangent, gate_weight, up_weight, down_weight_t):
        rows, d = tokens.shape
        ff = gate_weight.shape[1]
        scale = float(rows * n_rep * nx * cores) ** (-0.5)
        lines = d // (n_rep * cores)
        wb = tuple(ff - w for w in WIDTH_A)
        shapes = (((rows, d), BF16),) + (((lines, ff), F32),) * 3
        vmem = pl.BlockSpec(memory_space=pltpu.VMEM)
        dma = pltpu.SemaphoreType.DMA
        results = pl.pallas_call(
            functools.partial(body, nz, scale),
            out_shape=tuple(pltpu.VMEM(*s) for s in shapes),
            in_specs=[pl.BlockSpec(memory_space=pl.ANY)] * 5,
            out_specs=(vmem,) * 4,
            scratch_shapes=[
                pltpu.VMEM((nx, rows, d), BF16),
                pltpu.VMEM((2, nx, rows, d // 2), BF16),
                pltpu.VMEM((d, nx * rows), BF16),
                pltpu.VMEM((d, nx * rows), BF16),
                pltpu.VMEM((d, ff), BF16),
                pltpu.VMEM((d, ff), BF16),
                pltpu.VMEM((d, ff), BF16),
                pltpu.VMEM((ff, d), BF16),
                pltpu.VMEM((ff, d), BF16),
                pltpu.VMEM((nx, rows, ff), F32),
                pltpu.VMEM((nx, rows, ff), F32),
                pltpu.VMEM((nx, rows, ff), F32),
                pltpu.VMEM((nx * rows, ff), BF16),
                pltpu.VMEM((nx * rows, ff), BF16),
                pltpu.VMEM((nx * rows, ff), BF16),
                pltpu.VMEM((nx, rows, d), BF16),
                pltpu.VMEM((2, rows // 2, d), BF16),
                pltpu.VMEM((2, rows, d), BF16),
                pltpu.VMEM((3, nz, NY, cores, lines, ff), BF16),
                pltpu.VMEM((3, nz, NY, lines, ff), BF16),
                *[pltpu.VMEM((nz, NY, lines, w), BF16) for w in WIDTH_A],
                *[pltpu.VMEM((nz, NY, lines, w), BF16) for w in wb],
                *[pltpu.VMEM((3, nz, lines, w), BF16) for w in WIDTH_A],
                *[pltpu.VMEM((7, lines, w), BF16) for w in WIDTH_A],
                *[pltpu.VMEM((7, NY, lines, w), BF16) for w in wb],
                *[pltpu.VMEM((3, lines, w), BF16) for w in wb],
                dma((3 + 2 * nz,)),
                dma((3, 2, 3)),
                dma((3, 2, 3)),
                dma((3, nz // 2)),
                dma((3, nz // 2)),
                dma((6,)),
                dma((6,)),
                dma((12, 10)),
                dma((12, 10)),
            ],
            compiler_params=pltpu.CompilerParams(
                collective_id=0, has_side_effects=True, vmem_limit_bytes=60 * 1024 * 1024
            ),
        )(tokens, cotangent, gate_weight, up_weight, down_weight_t)
        return pl.pallas_call(
            written,
            out_shape=tuple(jax.ShapeDtypeStruct(*s) for s in shapes),
            in_specs=[vmem] * 4,
            out_specs=(pl.BlockSpec(memory_space=pltpu.HBM),) * 4,
            scratch_shapes=[dma((4,))],
        )(*[pltpu.with_memory_space_constraint(r, pltpu.VMEM) for r in results])

    return jax.shard_map(
        on_device,
        mesh=mesh,
        in_specs=(
            P(("rep", "fs", "tp"), None),
            P(("rep", "fs", "tp"), None),
            P(None, "fs"),
            P(None, "fs"),
            P(None, "fs"),
        ),
        out_specs=(
            P(("rep", "fs", "tp"), None),
            P(("rep", "tp"), "fs"),
            P(("rep", "tp"), "fs"),
            P(("rep", "tp"), "fs"),
        ),
        check_vma=False,
    )
```
